32 devices in a mesh: fs: 8 (over z, x), tp: 4 (over y, core).
Axes of the slice: x: 2, y: 2, z: 4, core: 2. Of those that a mesh axis runs over, the one named last changes fastest.
Arguments:
- tokens: bfloat16 [4096, 2048], P(('fs', 'tp')), may hold values from -6 to 6
- norm_gain: float32 [2048], P('fs'), may hold values from 0.1 to 1.9
- gate_proj: float32 [32, 2048, 512], P(None, 'fs', 'tp'), may hold values from -0.125 to 0.125
- up_proj: float32 [32, 2048, 512], P(None, 'fs', 'tp'), may hold values from -0.125 to 0.125
- down_proj: float32 [32, 512, 2048], P(None, 'fs', 'tp'), may hold values from -0.25 to 0.25
- expert_ids: int32 [4096, 2], P(('fs', 'tp')), may hold values from 0 to 31, as said below
- route_weight: float32 [4096, 2], P(('fs', 'tp')), may hold values from 0.05 to 1
Outputs:
- mixed: bfloat16 [4096, 2048], P(('fs', 'tp'))
- new_gate: bfloat16 [32, 2048, 512], P(('fs', 'tp'))
- new_up: bfloat16 [32, 2048, 512], P(('fs', 'tp'))
- new_down: bfloat16 [32, 512, 2048], P(('fs', 'tp'))
The draws below stay inside these ranges and needn't reach their ends.
Inputs may be any that keep to these rules, and one draw needn't show every extreme that they name: `expert_ids`: the two experts of a row differ and lie in one group of 4 consecutive experts. In each aligned block of 128 rows (the rows of one device) every group is named by exactly 16 rows, no expert by more than 16 rows, and one expert, the same in all blocks, by exactly 16 rows.
All inputs are finite; a program needn't handle non-finite values.
Results may differ from the reference program's by a relative error of at most 0.0087.
Values may be sent and summed in bfloat16 or wider, within the bound.
A program may use at most 128 MiB of HBM per device.

```python
import jax
import jax.numpy as jnp
from jax import lax

D = 2048
FF = 512
EPG = 4
TOK_DEV = 128
EXPERTS = 32
GROUPS = 8
CAP = 16
TOKENS = 4096


def draw_expert_ids(key, part):
    key_hot, key_blocks = jax.random.split(jax.random.fold_in(key, 17))
    hot_expert = jax.random.randint(key_hot, (), 0, EXPERTS)
    hot_group = hot_expert // EPG
    hot_slot = hot_expert % EPG

    def draw_block(block_key):
        key_order, key_first, key_second = jax.random.split(block_key, 3)
        position = jax.random.permutation(key_order, TOK_DEV)
        group_index = (hot_group + position // CAP) % GROUPS
        first_pick = jax.random.randint(key_first, (TOK_DEV,), 0, EPG)
        first_pick = jnp.where(position < CAP, hot_slot, first_pick)
        second_pick = (first_pick + jax.random.randint(key_second, (TOK_DEV,), 1, EPG)) % EPG
        return jnp.stack([group_index * EPG + first_pick, group_index * EPG + second_pick], axis=-1)
    block_keys = jax.random.split(key_blocks, TOKENS // TOK_DEV)
    return jax.vmap(draw_block)(block_keys).reshape(TOKENS, 2).astype(jnp.int32)


def shard_levels(key, dims, cuts, low, largest):
    def one(axis_at, parts):
        heights = jax.random.uniform(jax.random.fold_in(jax.random.fold_in(key, 6), axis_at), (parts,), jnp.float32, low / len(cuts), largest / len(cuts))
        return jnp.repeat(jnp.exp(heights), dims[axis_at] // parts).reshape((-1,) + (1,) * (len(dims) - axis_at - 1))

    gain = one(*cuts[0])
    for cut in cuts[1:]:
        gain = gain * one(*cut)
    return gain


def normal_values(key, shape, spread, most, cuts=(), held_as=jnp.bfloat16):
    array = jax.random.normal(key, shape, jnp.float32) * spread
    if len(cuts) > 0:
        array = shard_levels(key, shape, cuts, -0.22, 0.18) * array
    return jnp.clip(array, min=-most, max=most).astype(held_as)


def setup_inputs(seed: int = 0) -> dict:
    arg_keys = jax.random.split(jax.random.key(seed), 8)
    return {
        "tokens": normal_values(arg_keys[0], (TOKENS, D), 1.0, 6.0, ((0, 32),)),
        "norm_gain": jnp.clip(1.0 + 0.18 * jax.random.normal(arg_keys[1], (D,), jnp.float32), 0.1, 1.9),
        "gate_proj": normal_values(arg_keys[2], (EXPERTS, D, FF), D ** -0.5, 0.125, ((1, 8), (2, 4)), jnp.float32),
        "up_proj": normal_values(arg_keys[3], (EXPERTS, D, FF), D ** -0.5, 0.125, ((1, 8), (2, 4)), jnp.float32),
        "down_proj": normal_values(arg_keys[4], (EXPERTS, FF, D), FF ** -0.5, 0.25, ((1, 8), (2, 4)), jnp.float32),
        "expert_ids": draw_expert_ids(jax.random.fold_in(arg_keys[7], 71), 0),
        "route_weight": jnp.clip(0.05 + 0.95 * jax.random.uniform(arg_keys[6], (TOKENS, 2), jnp.float32) ** shard_levels(arg_keys[6], (TOKENS, 2), ((0, 32),), -0.2, 0.2), 0.05, 1.0),
    }


norm_eps = 1e-06

def reference(tokens, norm_gain, gate_proj, up_proj, down_proj, expert_ids, route_weight):
    row_scale = norm_gain[None, :, None]
    new_gate = (gate_proj * row_scale).astype(jnp.bfloat16)
    new_up = (up_proj * row_scale).astype(jnp.bfloat16)
    new_down = down_proj.astype(jnp.bfloat16)
    widened = tokens.astype(jnp.float32)
    normed = (widened * lax.rsqrt(lax.optimization_barrier(jnp.mean(widened * widened, axis=-1, keepdims=True)) + norm_eps)).astype(jnp.bfloat16)
    flat_ids = expert_ids.reshape(-1)
    flat_weight = route_weight.reshape(-1)
    most_rows = CAP * (TOKENS // TOK_DEV)

    def add_expert(expert, mixed_sum):
        named = flat_ids == expert
        pick_index = jnp.nonzero(named, size=most_rows, fill_value=0)[0]
        pick_count = jnp.sum(named.astype(jnp.int32))
        live_pick = jnp.arange(most_rows, dtype=jnp.int32) < pick_count
        token_rows = normed[pick_index // 2]
        gate_act = jnp.dot(token_rows, new_gate[expert], preferred_element_type=jnp.float32)
        up_act = jnp.dot(token_rows, new_up[expert], preferred_element_type=jnp.float32)
        hidden = (jax.nn.silu(gate_act) * up_act).astype(jnp.bfloat16)
        expert_out = jnp.dot(hidden, new_down[expert], preferred_element_type=jnp.float32).astype(jnp.bfloat16)
        weights = jnp.where(live_pick, flat_weight[pick_index], jnp.zeros((), jnp.float32))
        return mixed_sum.at[pick_index // 2].add(weights[:, None] * expert_out.astype(jnp.float32))
    mixed_sum = lax.fori_loop(0, EXPERTS, add_expert, jnp.zeros((TOKENS, D), jnp.float32))
    return (mixed_sum.astype(jnp.bfloat16), new_gate, new_up, new_down)
```

```python
import functools

import jax
import jax.numpy as jnp
from jax import lax
from jax.experimental import pallas as pl
from jax.experimental.pallas import tpu as pltpu
from jax.sharding import PartitionSpec as P

norm_eps = 1e-06
group_size = 4
extra_lanes = 128
MESH = pl.DeviceIdType.MESH


def shards_plain(tokens, norm_gain, gate_proj, up_proj, down_proj, expert_ids, route_weight):
    row_scale = norm_gain[None, :, None]
    gate_low = (gate_proj * row_scale).astype(jnp.bfloat16)
    up_low = (up_proj * row_scale).astype(jnp.bfloat16)
    down_low = down_proj.astype(jnp.bfloat16)
    width_fs = lax.axis_size("fs")
    width_tp = lax.axis_size("tp")

    def expand(matrix):
        return matrix.reshape((matrix.shape[0], 1) + matrix.shape[1:])

    def assemble(pieces):
        row_count, col_count = (pieces.shape[2], pieces.shape[3])
        tiled = pieces.reshape(width_fs, width_tp, row_count, col_count).transpose(0, 2, 1, 3)
        return tiled.reshape(1, width_fs * row_count, width_tp * col_count)

    arrived = (
        lax.all_to_all(expand(gate_low), ("fs", "tp"), split_axis=0, concat_axis=1, tiled=True),
        lax.all_to_all(expand(up_low), ("fs", "tp"), split_axis=0, concat_axis=1, tiled=True),
        lax.all_to_all(expand(down_low), ("fs", "tp"), split_axis=0, concat_axis=1, tiled=True),
    )
    new_gate, new_up, new_down = (assemble(arrived[0]), assemble(arrived[1]), assemble(arrived[2]))
    tok_count, width = tokens.shape
    experts = gate_proj.shape[0]
    slot_cap = 4 * tok_count // experts
    widened = tokens.astype(jnp.float32)
    normed = (
        widened * lax.rsqrt(jnp.mean(widened * widened, axis=-1, keepdims=True) + norm_eps)
    ).astype(jnp.bfloat16)
    flat_ids = expert_ids.reshape(-1)
    onehot = (flat_ids[:, None] == jnp.arange(experts, dtype=jnp.int32)[None, :]).astype(jnp.int32)
    slot_rank = jnp.sum(jnp.cumsum(onehot, axis=0) * onehot, axis=1) - 1
    slot_index = flat_ids * slot_cap + slot_rank
    source = (
        jnp.zeros((experts * slot_cap,), jnp.int32)
        .at[slot_index]
        .set(jnp.arange(2 * tok_count, dtype=jnp.int32) // 2 + 1)
    )
    filled = source > 0
    outgoing = jnp.where(
        filled[:, None], normed[jnp.maximum(source - 1, 0)], jnp.zeros((), jnp.bfloat16)
    )
    outgoing = outgoing.reshape(experts, slot_cap, width)
    arrived_rows = lax.all_to_all(outgoing, ("fs", "tp"), split_axis=0, concat_axis=0, tiled=True)
    flat_rows = arrived_rows.reshape(-1, width)
    gate_act = jnp.dot(flat_rows, new_gate[0], preferred_element_type=jnp.float32)
    up_act = jnp.dot(flat_rows, new_up[0], preferred_element_type=jnp.float32)
    hidden = (jax.nn.silu(gate_act) * up_act).astype(jnp.bfloat16)
    results = jnp.dot(hidden, new_down[0], preferred_element_type=jnp.float32).astype(jnp.bfloat16)
    returned = lax.all_to_all(
        results.reshape(arrived_rows.shape), ("fs", "tp"), split_axis=0, concat_axis=0, tiled=True
    )
    picked = returned.reshape(experts * slot_cap, width)[slot_index].reshape(tok_count, 2, width)
    mixed = jnp.sum(route_weight[:, :, None] * picked.astype(jnp.float32), axis=1).astype(
        jnp.bfloat16
    )
    return (mixed, new_gate, new_up, new_down)


def fused_kernel(
    n_fs, n_tp,
    x_in, ids_in, rw_in, gain_in, gate_in, up_in, down_in,
    gate_w, up_w, down_w, perm, fin_rx,
    x_ref, ids_ref, rw_ref, gain_ref,
    gate_st, up_st, down_st, gate_tx, up_tx, down_tx,
    tok_tx, rows, hidden, own, part_tx, part_rx, sum_tx, sum_rx, fin_tx,
    ld_sem, w_send, w_recv, tok_send, tok_recv, ex_send, ex_recv, red_send, red_recv,
    y_send, y_recv, fin_send, fin_recv, in_sem,
):
    f32, bf16 = jnp.float32, jnp.bfloat16
    fs, tp = lax.axis_index("fs"), lax.axis_index("tp")
    core = lax.rem(tp, 2)
    pair = tp // 2
    partner = tp + 1 - 2 * core
    across = lax.rem(tp + 2, n_tp)
    n_dev = n_fs * n_tp
    toks, width = x_ref.shape
    per = toks // n_fs
    srcs = (gate_in, up_in, down_in)
    stages = (gate_st, up_st, down_st)
    txs = (gate_tx, up_tx, down_tx)
    lands = (gate_w, up_w, down_w)

    barrier = pltpu.get_barrier_semaphore()

    @pl.loop(1, n_dev)
    def _(k):
        dev = lax.rem(fs * n_tp + tp + k, n_dev)
        pl.semaphore_signal(
            barrier, inc=1, device_id=(dev // n_tp, lax.rem(dev, n_tp)), device_id_type=MESH
        )

    quarter = n_fs // 4
    layer, col = fs // quarter, lax.rem(fs, quarter)
    half = layer // 2
    inner_far, outer_far, mate = 2 - half, 3 - 3 * half, 4 * half + 1 - layer

    def targets(layers):
        return [
            (at * quarter + lax.rem(col + 1 + i, quarter), at is layer and i == quarter - 1)
            for i in range(quarter)
            for at in layers
        ]

    orders = ((outer_far, inner_far), (mate, layer))
    plan = [
        (ms, goal) for at in orders for ms in ((0, 1), (2,)) for goal in targets(at)
    ]

    def load(m, tgt):
        at = pl.ds(tgt * n_tp, n_tp)
        return pltpu.make_async_copy(srcs[m].at[at], stages[m].at[at], ld_sem.at[m, tgt])

    small = [
        pltpu.make_async_copy(src, dst, in_sem.at[i])
        for i, (src, dst) in enumerate(
            ((gain_in, gain_ref), (x_in, x_ref), (ids_in, ids_ref), (rw_in, rw_ref))
        )
    ]
    small[0].start()
    for ms, (tgt, _) in plan:
        for m in ms:
            load(m, tgt).start()
    for copy in small[1:]:
        copy.start()

    lane = lax.broadcasted_iota(jnp.int32, (toks, extra_lanes), 1).astype(f32)
    lane_pick = jnp.where(lane < group_size, lane, lane - group_size)
    def as_columns(flat):
        spread_rows = jnp.concatenate([flat] * (8 // flat.shape[0]), axis=0)
        return jnp.transpose(spread_rows)

    def span(i):
        return pl.ds(pl.multiple_of(i * per, per), per)

    def spread(tx, land, send_sem, recv_sem):
        @pl.loop(1, n_fs)
        def _(j):
            tgt = lax.rem(fs + j, n_fs)
            pltpu.make_async_remote_copy(
                src_ref=tx.at[span(tgt)], dst_ref=land.at[span(fs)],
                send_sem=send_sem, recv_sem=recv_sem,
                device_id=(tgt, tp), device_id_type=MESH,
            ).start()

        pltpu.make_async_copy(tx.at[span(fs)], land.at[span(fs)], recv_sem).start()

    def all_sent(tx, sem, count):
        part = tx.at[pl.ds(0, count)]
        pltpu.make_async_copy(part, part, sem).wait()

    def all_here(land, sem):
        pltpu.make_async_copy(land, land, sem).wait()


    small[0].wait()
    gain = jnp.broadcast_to(as_columns(gain_ref[...])[:, 0:1], gate_in.shape[1:])

    def cast(ms, tgt):
        for m in ms:
            load(m, tgt).wait()

            @pl.loop(0, n_tp)
            def _(t):
                block = stages[m][tgt * n_tp + t]
                if m < 2:
                    block = block * gain
                txs[m][tgt * n_tp + t] = block.astype(bf16)

    def block_at(m):
        r, c = srcs[m].shape[1:]
        return lands[m].at[pl.ds(pl.multiple_of(fs * r, r), r), pl.ds(pl.multiple_of(tp * c, c), c)]

    def send(ms, tgt, first):
        for t in range(first, n_tp):
            to = lax.rem(tp + t, n_tp)
            for m in ms:
                pltpu.make_async_remote_copy(
                    src_ref=txs[m].at[tgt * n_tp + to], dst_ref=block_at(m),
                    send_sem=w_send.at[m], recv_sem=w_recv.at[m],
                    device_id=(tgt, to), device_id_type=MESH,
                ).start()

    def step_plan(first, last):
        for k in range(first, last):
            if k < len(plan):
                cast(plan[k][0], plan[k][1][0])
            if k > 0:
                ms, (tgt, same) = plan[k - 1]
                send(ms, tgt, 1 if same else 0)
                if same:
                    for m in ms:
                        pltpu.make_async_copy(
                            txs[m].at[fs * n_tp + tp], block_at(m), w_recv.at[m]
                        ).start()

    step_plan(0, 1)
    pl.semaphore_wait(barrier, n_dev - 1)
    step_plan(1, 3)

    for copy in small[1:]:
        copy.wait()
    x = x_ref[...].astype(f32)
    scale = lax.rsqrt(jnp.mean(x * x, axis=-1, keepdims=True) + norm_eps)
    normed = (x * scale).astype(bf16)
    idf = as_columns(ids_ref[...].astype(f32))
    grp = jnp.floor((idf + 0.5) * (1.0 / group_size))
    slot = lax.broadcasted_iota(jnp.int32, (toks, toks), 1).astype(f32)
    tok = lax.broadcasted_iota(jnp.int32, (toks, toks), 0).astype(f32)
    slot_grp = jnp.floor((slot + 0.5) * (1.0 / per))
    named = (grp[:, 0:1] == slot_grp).astype(f32)
    before = (slot < tok).astype(f32)
    rank = jnp.dot(before.astype(bf16), named.astype(bf16), preferred_element_type=f32)
    place = jnp.where(rank == slot - slot_grp * per, named, 0.0).astype(bf16)
    perm[...] = place
    local = idf - grp * group_size
    rw = as_columns(rw_ref[...])
    wv = jnp.where(local[:, 0:1] == lane_pick, rw[:, 0:1], 0.0) + jnp.where(
        local[:, 1:2] == lane_pick, rw[:, 1:2], 0.0
    )
    high = wv.astype(bf16)
    low = (wv - high.astype(f32)).astype(bf16)
    aug = jnp.where(
        lane < group_size,
        high.astype(f32),
        jnp.where(lane < 2 * group_size, low.astype(f32), 0.0),
    ).astype(bf16)
    by_slot = (((0,), (0,)), ((), ()))
    tok_tx[:, 0:width] = lax.dot_general(
        place, normed, by_slot, preferred_element_type=f32
    ).astype(bf16)
    tok_tx[:, width:] = lax.dot_general(
        place, aug, by_slot, preferred_element_type=f32
    ).astype(bf16)
    spread(tok_tx, rows.at[tp], tok_send, tok_recv)

    step_plan(3, len(plan) + 1)

    def swap(src, dst, to, send_sem, recv_sem):
        return pltpu.make_async_remote_copy(
            src_ref=src, dst_ref=dst, send_sem=send_sem, recv_sem=recv_sem,
            device_id=(fs, to), device_id_type=MESH,
        )

    all_here(rows.at[tp], tok_recv)
    cross = swap(rows.at[tp], rows.at[tp], across, ex_send.at[0], ex_recv.at[0])
    cross.start()
    near = swap(rows.at[tp], rows.at[tp], partner, ex_send.at[1], ex_recv.at[1])
    near.start()
    cross.wait()
    far = swap(rows.at[across], rows.at[across], partner, ex_send.at[2], ex_recv.at[2])
    far.start()
    near.wait()
    far.wait()

    for m in (0, 1):
        all_here(lands[m], w_recv.at[m])

    @pl.loop(0, n_tp)
    def _(q):
        block = rows[q, :, 0:width]
        g = jnp.dot(block, gate_w[...], preferred_element_type=f32)
        u = jnp.dot(block, up_w[...], preferred_element_type=f32)
        hidden[q] = (g / (1.0 + jnp.exp(-g)) * u).astype(bf16)

    all_here(down_w, w_recv.at[2])

    tpf = tp.astype(f32)

    def partial(q):
        w = jnp.sum(
            jnp.where(lane_pick == tpf, rows[q, :, width:].astype(f32), 0.0),
            axis=-1, keepdims=True,
        )
        return jnp.dot(hidden[q], down_w[...], preferred_element_type=f32) * w

    def reduce_near(i, p):
        return swap(part_tx.at[i], part_rx.at[i], partner, red_send.at[i], red_recv.at[i])

    def give(i, side):
        part_tx[i] = partial(side * 2 + 1 - core).astype(bf16)
        reduce_near(i, partner).start()
        own[i] = partial(side * 2 + core)
        reduce_near(i, partner).wait()
        own[i] = own[i] + part_rx[i].astype(f32)

    pieces = 4
    step = n_fs // pieces

    def piece(p):
        return lax.rem(half * 2 + 2 + p, pieces)

    def piece_rows(p):
        return pl.ds(pl.multiple_of(piece(p) * step * per, step * per), step * per)

    def over(p):
        at = piece_rows(p)
        return swap(sum_tx.at[at], sum_rx.at[at], across, y_send.at[p], y_recv.at[p])

    give(0, 1 - pair)
    for p in range(pieces):
        at = piece_rows(p)
        sum_tx[at] = own[0, at].astype(bf16)
    for p in range(pieces):
        over(p).start()
    give(1, pair)

    def give_back(p):
        for i in range(step):
            to = piece(p) * step + i

            @pl.when(to != fs)
            def _():
                pltpu.make_async_remote_copy(
                    src_ref=fin_tx.at[span(to)], dst_ref=fin_rx.at[span(fs)],
                    send_sem=fin_send, recv_sem=fin_recv,
                    device_id=(to, tp), device_id_type=MESH,
                ).start()

            @pl.when(to == fs)
            def _():
                pltpu.make_async_copy(
                    fin_tx.at[span(fs)], fin_rx.at[span(fs)], fin_recv
                ).start()

    for p in range(pieces):
        over(p).wait()
        at = piece_rows(p)
        fin_tx[at] = (own[1, at] + sum_rx[at].astype(f32)).astype(bf16)
        give_back(p)
    for m in range(3):
        all_sent(txs[m], w_send.at[m], n_dev - 1)
    all_sent(tok_tx, tok_send, toks - per)
    all_sent(fin_tx, fin_send, toks - per)
    all_here(fin_rx, fin_recv)


def write_kernel(perm, fin_rx, gate, up, down, mixed_ref, gate_out, up_out, down_out, sem):
    moves = ((gate, gate_out), (up, up_out), (down, down_out))

    def put(m):
        return pltpu.make_async_copy(moves[m][0], moves[m][1], sem.at[m])

    for m in range(3):
        put(m).start()
    mixed_ref[...] = jnp.dot(
        perm[...], fin_rx[...], preferred_element_type=jnp.float32
    ).astype(jnp.bfloat16)
    for m in range(3):
        put(m).wait()


def shards_fused(n_fs, n_tp, tokens, norm_gain, gate_proj, up_proj, down_proj, expert_ids, route_weight):
    f32, bf16 = jnp.float32, jnp.bfloat16
    n_dev = n_fs * n_tp
    toks, width = tokens.shape
    _, gr, gc = gate_proj.shape
    _, dr, dc = down_proj.shape
    inner = gc * n_tp
    wide = width + extra_lanes
    vmem = pl.BlockSpec(memory_space=pltpu.VMEM)
    hbm = pl.BlockSpec(memory_space=pltpu.HBM)
    dma = pltpu.SemaphoreType.DMA
    new_gate, new_up, new_down, perm, returned = pl.pallas_call(
        functools.partial(fused_kernel, n_fs, n_tp),
        out_shape=(
            pltpu.VMEM((width, inner), bf16),
            pltpu.VMEM((width, inner), bf16),
            pltpu.VMEM((inner, width), bf16),
            pltpu.VMEM((toks, toks), bf16),
            pltpu.VMEM((toks, width), bf16),
        ),
        in_specs=[hbm] * 7,
        out_specs=(vmem,) * 5,
        scratch_shapes=[
            pltpu.VMEM(tokens.shape, bf16),
            pltpu.VMEM((2, toks), jnp.int32),
            pltpu.VMEM((2, toks), f32),
            pltpu.VMEM((1, gr), f32),
            pltpu.VMEM((n_dev, gr, gc), f32),
            pltpu.VMEM((n_dev, gr, gc), f32),
            pltpu.VMEM((n_dev, dr, dc), f32),
            pltpu.VMEM((n_dev, gr, gc), bf16),
            pltpu.VMEM((n_dev, gr, gc), bf16),
            pltpu.VMEM((n_dev, dr, dc), bf16),
            pltpu.VMEM((toks, wide), bf16),
            pltpu.VMEM((n_tp, toks, wide), bf16),
            pltpu.VMEM((n_tp, toks, inner), bf16),
            pltpu.VMEM((2, toks, width), f32),
            pltpu.VMEM((2, toks, width), bf16),
            pltpu.VMEM((2, toks, width), bf16),
            pltpu.VMEM((toks, width), bf16),
            pltpu.VMEM((toks, width), bf16),
            pltpu.VMEM((toks, width), bf16),
            dma((3, n_fs)), dma((3,)), dma((3,)), dma, dma, dma((3,)), dma((3,)),
            dma((2,)), dma((2,)), dma((4,)), dma((4,)), dma, dma, dma((4,)),
        ],
        compiler_params=pltpu.CompilerParams(
            collective_id=0, has_side_effects=True, vmem_limit_bytes=40 * 1024 * 1024
        ),
    )(*(
        pltpu.with_memory_space_constraint(a, pltpu.HBM)
        for a in (
            tokens, expert_ids.T, route_weight.T, norm_gain[None, :], gate_proj, up_proj, down_proj
        )
    ))
    mixed, new_gate, new_up, new_down = pl.pallas_call(
        write_kernel,
        out_shape=(
            jax.ShapeDtypeStruct((toks, width), bf16),
            jax.ShapeDtypeStruct((width, inner), bf16),
            jax.ShapeDtypeStruct((width, inner), bf16),
            jax.ShapeDtypeStruct((inner, width), bf16),
        ),
        in_specs=[vmem] * 5,
        out_specs=(vmem, hbm, hbm, hbm),
        scratch_shapes=[dma((3,))],
        compiler_params=pltpu.CompilerParams(vmem_limit_bytes=16 * 1024 * 1024),
    )(perm, returned, new_gate, new_up, new_down)
    return mixed, new_gate[None], new_up[None], new_down[None]


def shards(n_fs, n_tp, *args):
    tokens, _, gate_proj, _, down_proj = args[:5]
    toks, experts = tokens.shape[0], gate_proj.shape[0]
    whole_tiles = (
        n_tp == group_size
        and experts == n_fs * n_tp
        and toks % (16 * n_fs) == 0
        and n_fs % 4 == 0
        and gate_proj.shape[2] % 128 == 0
        and down_proj.shape[2] % 128 == 0
        and gate_proj.shape[1] % 16 == 0
        and down_proj.shape[1] % 16 == 0
    )
    if whole_tiles:
        return shards_fused(n_fs, n_tp, *args)
    return shards_plain(*args)


def solution(mesh):
    in_specs = (
        P(("fs", "tp"), None),
        P("fs"),
        P(None, "fs", "tp"),
        P(None, "fs", "tp"),
        P(None, "fs", "tp"),
        P(("fs", "tp"), None),
        P(("fs", "tp"), None),
    )
    out_specs = (
        P(("fs", "tp"), None),
        P(("fs", "tp"), None, None),
        P(("fs", "tp"), None, None),
        P(("fs", "tp"), None, None),
    )
    body = functools.partial(shards, mesh.shape["fs"], mesh.shape["tp"])
    return jax.shard_map(body, mesh=mesh, in_specs=in_specs, out_specs=out_specs, check_vma=False)
```

```python
import functools

import jax
import jax.numpy as jnp
from jax import lax
from jax.experimental import pallas as pl
from jax.experimental.pallas import tpu as pltpu
from jax.sharding import PartitionSpec as P

norm_eps = 1e-06
group_size = 4
lanes = 128
MESH = pl.DeviceIdType.MESH


def shards_plain(tokens, norm_gain, gate_proj, up_proj, down_proj, expert_ids, route_weight):
    row_scale = norm_gain[None, :, None]
    gate_low = (gate_proj * row_scale).astype(jnp.bfloat16)
    up_low = (up_proj * row_scale).astype(jnp.bfloat16)
    down_low = down_proj.astype(jnp.bfloat16)
    width_fs = lax.axis_size("fs")
    width_tp = lax.axis_size("tp")

    def expand(matrix):
        return matrix.reshape((matrix.shape[0], 1) + matrix.shape[1:])

    def assemble(pieces):
        row_count, col_count = (pieces.shape[2], pieces.shape[3])
        tiled = pieces.reshape(width_fs, width_tp, row_count, col_count).transpose(0, 2, 1, 3)
        return tiled.reshape(1, width_fs * row_count, width_tp * col_count)

    arrived = (
        lax.all_to_all(expand(gate_low), ("fs", "tp"), split_axis=0, concat_axis=1, tiled=True),
        lax.all_to_all(expand(up_low), ("fs", "tp"), split_axis=0, concat_axis=1, tiled=True),
        lax.all_to_all(expand(down_low), ("fs", "tp"), split_axis=0, concat_axis=1, tiled=True),
    )
    new_gate, new_up, new_down = (assemble(arrived[0]), assemble(arrived[1]), assemble(arrived[2]))
    tok_count, width = tokens.shape
    experts = gate_proj.shape[0]
    slot_cap = 4 * tok_count // experts
    widened = tokens.astype(jnp.float32)
    normed = (
        widened * lax.rsqrt(jnp.mean(widened * widened, axis=-1, keepdims=True) + norm_eps)
    ).astype(jnp.bfloat16)
    flat_ids = expert_ids.reshape(-1)
    onehot = (flat_ids[:, None] == jnp.arange(experts, dtype=jnp.int32)[None, :]).astype(jnp.int32)
    slot_rank = jnp.sum(jnp.cumsum(onehot, axis=0) * onehot, axis=1) - 1
    slot_index = flat_ids * slot_cap + slot_rank
    source = (
        jnp.zeros((experts * slot_cap,), jnp.int32)
        .at[slot_index]
        .set(jnp.arange(2 * tok_count, dtype=jnp.int32) // 2 + 1)
    )
    filled = source > 0
    outgoing = jnp.where(
        filled[:, None], normed[jnp.maximum(source - 1, 0)], jnp.zeros((), jnp.bfloat16)
    )
    outgoing = outgoing.reshape(experts, slot_cap, width)
    arrived_rows = lax.all_to_all(outgoing, ("fs", "tp"), split_axis=0, concat_axis=0, tiled=True)
    flat_rows = arrived_rows.reshape(-1, width)
    gate_act = jnp.dot(flat_rows, new_gate[0], preferred_element_type=jnp.float32)
    up_act = jnp.dot(flat_rows, new_up[0], preferred_element_type=jnp.float32)
    hidden = (jax.nn.silu(gate_act) * up_act).astype(jnp.bfloat16)
    results = jnp.dot(hidden, new_down[0], preferred_element_type=jnp.float32).astype(jnp.bfloat16)
    returned = lax.all_to_all(
        results.reshape(arrived_rows.shape), ("fs", "tp"), split_axis=0, concat_axis=0, tiled=True
    )
    picked = returned.reshape(experts * slot_cap, width)[slot_index].reshape(tok_count, 2, width)
    mixed = jnp.sum(route_weight[:, :, None] * picked.astype(jnp.float32), axis=1).astype(
        jnp.bfloat16
    )
    return (mixed, new_gate, new_up, new_down)


def fused_kernel(
    n_fs, n_tp,
    x_in, ids_in, rw_in, gain_in, gate_in, up_in, down_in,
    gate_w, up_w, down_w, perm, fin_rx,
    x_ref, ids_ref, rw_ref, gain_ref,
    gate_st, up_st, down_st, gate_tx, up_tx, down_tx,
    tok_tx, rows, wt_tx, wt_rx, wcol, hidden, own,
    part_tx, part_rx, sum_tx, sum_rx, fin_tx,
    in_sem, ld_sem, w_send, w_recv, tok_send, tok_recv, wt_send, wt_recv, ex_send, ex_recv,
    red_send, red_recv, y_send, y_recv, fin_send, fin_recv,
):
    f32, bf16 = jnp.float32, jnp.bfloat16
    fs, tp = lax.axis_index("fs"), lax.axis_index("tp")
    core = lax.rem(tp, 2)
    pair = tp // 2
    partner = tp + 1 - 2 * core
    across = lax.rem(tp + 2, n_tp)
    n_dev = n_fs * n_tp
    toks, width = x_ref.shape
    per = toks // n_fs
    d_rows, d_cols = down_in.shape[1:]
    chunks = d_cols // lanes
    srcs = (gate_in, up_in, down_in)
    stages = (gate_st, up_st, down_st)
    txs = (gate_tx, up_tx, down_tx)
    lands = (gate_w, up_w, down_w)

    barrier = pltpu.get_barrier_semaphore()

    @pl.loop(1, n_dev)
    def _(k):
        dev = lax.rem(fs * n_tp + tp + k, n_dev)
        pl.semaphore_signal(
            barrier, inc=1, device_id=(dev // n_tp, lax.rem(dev, n_tp)), device_id_type=MESH
        )

    quarter = n_fs // 4
    layer, col = fs // quarter, lax.rem(fs, quarter)
    half = layer // 2
    inner_far, outer_far, mate = 2 - half, 3 - 3 * half, 4 * half + 1 - layer

    def targets(layers):
        return [
            (at * quarter + lax.rem(col + 1 + i, quarter), at is layer and i == quarter - 1)
            for i in range(quarter)
            for at in layers
        ]

    far, close = targets((outer_far, inner_far)), targets((mate, layer))
    ahead = 1
    plan = far[:ahead] + close + far[ahead:]

    def load(m, tgt):
        at = pl.ds(tgt * n_tp, n_tp)
        return pltpu.make_async_copy(srcs[m].at[at], stages[m].at[at], ld_sem.at[m, tgt])

    small = [
        pltpu.make_async_copy(src, dst, in_sem.at[i])
        for i, (src, dst) in enumerate(
            ((gain_in, gain_ref), (x_in, x_ref), (ids_in, ids_ref), (rw_in, rw_ref))
        )
    ]
    small[0].start()
    for m in (0, 1):
        load(m, plan[0][0]).start()

    lane_id = lax.broadcasted_iota(jnp.int32, (toks, lanes), 1)
    row_id = lax.broadcasted_iota(jnp.int32, (toks, lanes), 0)
    in_group = lax.rem(row_id, per)
    span_lanes = group_size * per

    def as_columns(flat):
        spread_rows = jnp.concatenate([flat] * (8 // flat.shape[0]), axis=0)
        return jnp.transpose(spread_rows)

    def span(i):
        return pl.ds(pl.multiple_of(i * per, per), per)

    def all_sent(part, sem):
        pltpu.make_async_copy(part, part, sem).wait()

    def all_here(land, sem):
        pltpu.make_async_copy(land, land, sem).wait()

    small[0].wait()
    gain = jnp.broadcast_to(as_columns(gain_ref[...])[:, 0:1], gate_in.shape[1:])

    def cast(ms, tgt):
        for m in ms:
            load(m, tgt).wait()

            @pl.loop(0, n_tp)
            def _(t):
                block = stages[m][tgt * n_tp + t]
                if m < 2:
                    block = block * gain
                txs[m][tgt * n_tp + t] = block.astype(bf16)

    def block_at(m):
        r, c = srcs[m].shape[1:]
        return lands[m].at[pl.ds(pl.multiple_of(fs * r, r), r), pl.ds(pl.multiple_of(tp * c, c), c)]

    def send(tgt, same):
        for t in range(1 if same else 0, n_tp):
            to = lax.rem(tp + t, n_tp)
            for m in (0, 1):
                pltpu.make_async_remote_copy(
                    src_ref=txs[m].at[tgt * n_tp + to], dst_ref=block_at(m),
                    send_sem=w_send.at[m], recv_sem=w_recv.at[m],
                    device_id=(tgt, to), device_id_type=MESH,
                ).start()
        if same:
            for m in (0, 1):
                pltpu.make_async_copy(
                    txs[m].at[fs * n_tp + tp], block_at(m), w_recv.at[m]
                ).start()

    def step_plan(first, last):
        for k in range(first, last):
            if k < len(plan):
                cast((0, 1), plan[k][0])
            if k > 0:
                send(*plan[k - 1])

    def chunk_block(k):
        return down_w.at[
            pl.ds(pl.multiple_of(fs * d_rows, d_rows), d_rows),
            pl.ds(pl.multiple_of(tp * d_cols + k * lanes, lanes), lanes),
        ]

    def send_chunk(k):
        for tgt, same in close + far:
            for t in range(1 if same else 0, n_tp):
                to = lax.rem(tp + t, n_tp)
                pltpu.make_async_remote_copy(
                    src_ref=down_tx.at[tgt * n_tp + to, :, pl.ds(k * lanes, lanes)],
                    dst_ref=chunk_block(k),
                    send_sem=w_send.at[2 + k], recv_sem=w_recv.at[2 + k],
                    device_id=(tgt, to), device_id_type=MESH,
                ).start()
            if same:
                pltpu.make_async_copy(
                    down_tx.at[fs * n_tp + tp, :, pl.ds(k * lanes, lanes)],
                    chunk_block(k), w_recv.at[2 + k],
                ).start()

    step_plan(0, 1)
    for copy in small[1:]:
        copy.start()
    for ms in ((0, 1), (2,)):
        for tgt, _ in plan[1:] if ms[0] == 0 else plan:
            for m in ms:
                load(m, tgt).start()
    pl.semaphore_wait(barrier, n_dev - 1)
    step_plan(1, ahead + 1)

    for copy in small[1:]:
        copy.wait()
    x = x_ref[...].astype(f32)
    scale = lax.rsqrt(jnp.mean(x * x, axis=-1, keepdims=True) + norm_eps)
    normed = (x * scale).astype(bf16)
    idf = as_columns(ids_ref[...].astype(f32))
    grp = jnp.floor((idf + 0.5) * (1.0 / group_size))
    slot = lax.broadcasted_iota(jnp.int32, (toks, toks), 1).astype(f32)
    tok = lax.broadcasted_iota(jnp.int32, (toks, toks), 0).astype(f32)
    slot_grp = jnp.floor((slot + 0.5) * (1.0 / per))
    named = (grp[:, 0:1] == slot_grp).astype(f32)
    before = (slot < tok).astype(f32)
    rank = jnp.dot(before.astype(bf16), named.astype(bf16), preferred_element_type=f32)
    place = jnp.where(rank == slot - slot_grp * per, named, 0.0).astype(bf16)
    perm[...] = place
    by_slot = (((0,), (0,)), ((), ()))
    tok_tx[...] = lax.dot_general(
        place, normed, by_slot, preferred_element_type=f32
    ).astype(bf16)

    @pl.loop(1, n_fs)
    def _(j):
        tgt = lax.rem(fs + j, n_fs)
        pltpu.make_async_remote_copy(
            src_ref=tok_tx.at[span(tgt)], dst_ref=rows.at[tp, span(fs)],
            send_sem=tok_send, recv_sem=tok_recv,
            device_id=(tgt, tp), device_id_type=MESH,
        ).start()

    pltpu.make_async_copy(tok_tx.at[span(fs)], rows.at[tp, span(fs)], tok_recv).start()

    lane_pick = (lax.rem(lane_id, span_lanes) // per).astype(f32)
    local = idf - grp * group_size
    rw = as_columns(rw_ref[...])
    wv = jnp.where(local[:, 0:1] == lane_pick, rw[:, 0:1], 0.0) + jnp.where(
        local[:, 1:2] == lane_pick, rw[:, 1:2], 0.0
    )
    high = wv.astype(bf16).astype(f32)
    aug = jnp.where(lane_id < span_lanes, high, wv - high).astype(bf16)
    by_row = lax.dot_general(place, aug, by_slot, preferred_element_type=f32)
    by_row = jnp.where(lax.rem(lane_id, per) == in_group, by_row, 0.0)
    wt_tx[...] = jnp.sum(by_row.reshape(n_fs, per, lanes), axis=1, keepdims=True)

    @pl.loop(1, n_dev)
    def _(k):
        dev = lax.rem(fs * n_tp + tp + k, n_dev)
        tgt = dev // n_tp
        pltpu.make_async_remote_copy(
            src_ref=wt_tx.at[tgt], dst_ref=wt_rx.at[tp, fs],
            send_sem=wt_send, recv_sem=wt_recv,
            device_id=(tgt, lax.rem(dev, n_tp)), device_id_type=MESH,
        ).start()

    pltpu.make_async_copy(wt_tx.at[fs], wt_rx.at[tp, fs], wt_recv).start()

    step_plan(ahead + 1, len(plan) + 1)
    for tgt, _ in plan:
        cast((2,), tgt)
    for k in range(chunks - 1):
        send_chunk(k)

    def swap(src, dst, to, send_sem, recv_sem):
        return pltpu.make_async_remote_copy(
            src_ref=src, dst_ref=dst, send_sem=send_sem, recv_sem=recv_sem,
            device_id=(fs, to), device_id_type=MESH,
        )

    all_here(rows.at[tp], tok_recv)
    cross = swap(rows.at[tp], rows.at[tp], across, ex_send.at[0], ex_recv.at[0])
    cross.start()
    near = swap(rows.at[tp], rows.at[tp], partner, ex_send.at[1], ex_recv.at[1])
    near.start()
    cross.wait()
    other = swap(rows.at[across], rows.at[across], partner, ex_send.at[2], ex_recv.at[2])
    other.start()
    near.wait()
    other.wait()
    all_here(wt_rx, wt_recv)
    mine = lax.rem(lane_id, span_lanes) == tp * per + in_group

    @pl.loop(0, n_tp)
    def _(q):
        w = jnp.broadcast_to(wt_rx[q], (n_fs, per, lanes)).reshape(toks, lanes)
        wcol[q] = jnp.broadcast_to(
            jnp.sum(jnp.where(mine, w, 0.0), axis=-1, keepdims=True), (toks, lanes)
        )

    for m in (0, 1):
        all_here(lands[m], w_recv.at[m])

    @pl.loop(0, n_tp)
    def _(q):
        g = jnp.dot(rows[q], gate_w[...], preferred_element_type=f32)
        u = jnp.dot(rows[q], up_w[...], preferred_element_type=f32)
        hidden[q] = (g / (1.0 + jnp.exp(-g)) * u).astype(bf16)

    pieces = 4
    step = n_fs // pieces

    def piece(p):
        return lax.rem(half * 2 + 2 + p, pieces)

    def piece_rows(p):
        return pl.ds(pl.multiple_of(piece(p) * step * per, step * per), step * per)

    def reduce_near(k):
        return swap(part_tx.at[k], part_rx.at[k], partner, red_send.at[k], red_recv.at[k])

    def over(k, p):
        at = piece_rows(p)
        return swap(
            sum_tx.at[k, at], sum_rx.at[k, at], across, y_send.at[k, p], y_recv.at[k, p]
        )

    def multiply(k):
        columns = jnp.concatenate(
            [down_w[:, pl.ds(t * d_cols + k * lanes, lanes)] for t in range(n_tp)], axis=1
        )

        def partial(q):
            w = jnp.concatenate([wcol[q]] * n_tp, axis=1)
            return jnp.dot(hidden[q], columns, preferred_element_type=f32) * w

        for side in range(2):
            part_tx[k, side] = partial(side * 2 + 1 - core).astype(bf16)
        reduce_near(k).start()
        own[k, 0] = partial((1 - pair) * 2 + core)
        own[k, 1] = partial(pair * 2 + core)

    def cross_over(k):
        reduce_near(k).wait()
        for p in range(pieces):
            at = piece_rows(p)
            sum_tx[k, at] = (own[k, 0, at] + part_rx[k, 1 - pair, at].astype(f32)).astype(bf16)
            over(k, p).start()

    def give_back(k):
        for p in range(pieces):
            at = piece_rows(p)
            own_part = own[k, 1, at] + part_rx[k, pair, at].astype(f32)
            over(k, p).wait()
            fin_tx[k, at] = (own_part + sum_rx[k, at].astype(f32)).astype(bf16)
            for i in range(step):
                to = piece(p) * step + i

                @pl.when(to != fs)
                def _():
                    pltpu.make_async_remote_copy(
                        src_ref=fin_tx.at[k, span(to)], dst_ref=fin_rx.at[k, span(fs)],
                        send_sem=fin_send, recv_sem=fin_recv,
                        device_id=(to, tp), device_id_type=MESH,
                    ).start()

                @pl.when(to == fs)
                def _():
                    pltpu.make_async_copy(
                        fin_tx.at[k, span(fs)], fin_rx.at[k, span(fs)], fin_recv
                    ).start()

    chunk_area = down_w.at[:, pl.ds(0, n_tp * lanes)]
    for k in range(chunks):
        all_here(chunk_area, w_recv.at[2 + k])
        multiply(k)
        if k > 0:
            give_back(k - 1)
        if k == 1:
            send_chunk(chunks - 1)
        cross_over(k)
    give_back(chunks - 1)

    for m in (0, 1):
        all_sent(txs[m].at[pl.ds(0, n_dev - 1)], w_send.at[m])
    for k in range(chunks):
        all_sent(down_tx.at[pl.ds(0, n_dev - 1), :, pl.ds(0, lanes)], w_send.at[2 + k])
    all_sent(tok_tx.at[pl.ds(0, toks - per)], tok_send)
    all_sent(wt_rx.at[0, pl.ds(0, n_fs - 1)], wt_send)
    for _ in range(n_tp - 1):
        all_sent(wt_rx.at[0], wt_send)
    all_sent(fin_tx.at[:, pl.ds(0, toks - per)], fin_send)
    all_here(fin_rx, fin_recv)


def write_kernel(perm, fin_rx, gate, up, down, mixed_out, gate_out, up_out, down_out, mixed, sem):
    chunks, _, wide = fin_rx.shape
    blocks = wide // lanes
    moves = ((gate, gate_out), (up, up_out), (down, down_out), (mixed, mixed_out))

    def put(m):
        return pltpu.make_async_copy(moves[m][0], moves[m][1], sem.at[m])

    for m in range(3):
        put(m).start()
    for k in range(chunks):
        part = jnp.dot(
            perm[...], fin_rx[k], preferred_element_type=jnp.float32
        ).astype(jnp.bfloat16)
        for t in range(blocks):
            mixed[:, pl.ds((t * chunks + k) * lanes, lanes)] = part[:, t * lanes:(t + 1) * lanes]
    put(3).start()
    for m in range(4):
        put(m).wait()


def shards_fused(n_fs, n_tp, tokens, norm_gain, gate_proj, up_proj, down_proj, expert_ids, route_weight):
    f32, bf16 = jnp.float32, jnp.bfloat16
    n_dev = n_fs * n_tp
    toks, width = tokens.shape
    _, gr, gc = gate_proj.shape
    _, dr, dc = down_proj.shape
    inner = gc * n_tp
    chunks, wide = dc // lanes, n_tp * lanes
    vmem = pl.BlockSpec(memory_space=pltpu.VMEM)
    hbm = pl.BlockSpec(memory_space=pltpu.HBM)
    dma = pltpu.SemaphoreType.DMA
    new_gate, new_up, new_down, perm, returned = pl.pallas_call(
        functools.partial(fused_kernel, n_fs, n_tp),
        out_shape=(
            pltpu.VMEM((width, inner), bf16),
            pltpu.VMEM((width, inner), bf16),
            pltpu.VMEM((inner, width), bf16),
            pltpu.VMEM((toks, toks), bf16),
            pltpu.VMEM((chunks, toks, wide), bf16),
        ),
        in_specs=[hbm] * 7,
        out_specs=(vmem,) * 5,
        scratch_shapes=[
            pltpu.VMEM(tokens.shape, bf16),
            pltpu.VMEM((2, toks), jnp.int32),
            pltpu.VMEM((2, toks), f32),
            pltpu.VMEM((1, gr), f32),
            pltpu.VMEM((n_dev, gr, gc), f32),
            pltpu.VMEM((n_dev, gr, gc), f32),
            pltpu.VMEM((n_dev, dr, dc), f32),
            pltpu.VMEM((n_dev, gr, gc), bf16),
            pltpu.VMEM((n_dev, gr, gc), bf16),
            pltpu.VMEM((n_dev, dr, dc), bf16),
            pltpu.VMEM((toks, width), bf16),
            pltpu.VMEM((n_tp, toks, width), bf16),
            pltpu.VMEM((n_fs, 1, lanes), f32),
            pltpu.VMEM((n_tp, n_fs, 1, lanes), f32),
            pltpu.VMEM((n_tp, toks, lanes), f32),
            pltpu.VMEM((n_tp, toks, inner), bf16),
            pltpu.VMEM((chunks, 2, toks, wide), f32),
            pltpu.VMEM((chunks, 2, toks, wide), bf16),
            pltpu.VMEM((chunks, 2, toks, wide), bf16),
            pltpu.VMEM((chunks, toks, wide), bf16),
            pltpu.VMEM((chunks, toks, wide), bf16),
            pltpu.VMEM((chunks, toks, wide), bf16),
            dma((4,)), dma((3, n_fs)), dma((2 + chunks,)), dma((2 + chunks,)), dma, dma, dma, dma,
            dma((3,)), dma((3,)), dma((chunks,)), dma((chunks,)), dma((chunks, 4)),
            dma((chunks, 4)), dma, dma,
        ],
        compiler_params=pltpu.CompilerParams(
            collective_id=0, has_side_effects=True, vmem_limit_bytes=46 * 1024 * 1024
        ),
    )(*(
        pltpu.with_memory_space_constraint(a, pltpu.HBM)
        for a in (
            tokens, expert_ids.T, route_weight.T, norm_gain[None, :], gate_proj, up_proj, down_proj
        )
    ))
    mixed, new_gate, new_up, new_down = pl.pallas_call(
        write_kernel,
        out_shape=(
            jax.ShapeDtypeStruct((toks, width), bf16),
            jax.ShapeDtypeStruct((width, inner), bf16),
            jax.ShapeDtypeStruct((width, inner), bf16),
            jax.ShapeDtypeStruct((inner, width), bf16),
        ),
        in_specs=[vmem] * 5,
        out_specs=(hbm,) * 4,
        scratch_shapes=[pltpu.VMEM((toks, width), bf16), dma((4,))],
        compiler_params=pltpu.CompilerParams(vmem_limit_bytes=16 * 1024 * 1024),
    )(perm, returned, new_gate, new_up, new_down)
    return mixed, new_gate[None], new_up[None], new_down[None]


def shards(n_fs, n_tp, *args):
    tokens, _, gate_proj, _, down_proj = args[:5]
    toks, experts = tokens.shape[0], gate_proj.shape[0]
    whole_tiles = (
        n_tp == group_size
        and experts == n_fs * n_tp
        and toks % (16 * n_fs) == 0
        and n_fs % 4 == 0
        and gate_proj.shape[2] % 128 == 0
        and down_proj.shape[2] % 128 == 0
        and gate_proj.shape[1] % 16 == 0
        and down_proj.shape[1] % 16 == 0
        and 2 * group_size * toks == lanes * n_fs
    )
    if whole_tiles:
        return shards_fused(n_fs, n_tp, *args)
    return shards_plain(*args)


def solution(mesh):
    in_specs = (
        P(("fs", "tp"), None),
        P("fs"),
        P(None, "fs", "tp"),
        P(None, "fs", "tp"),
        P(None, "fs", "tp"),
        P(("fs", "tp"), None),
        P(("fs", "tp"), None),
    )
    out_specs = (
        P(("fs", "tp"), None),
        P(("fs", "tp"), None, None),
        P(("fs", "tp"), None, None),
        P(("fs", "tp"), None, None),
    )
    body = functools.partial(shards, mesh.shape["fs"], mesh.shape["tp"])
    return jax.shard_map(body, mesh=mesh, in_specs=in_specs, out_specs=out_specs, check_vma=False)
```

```python
import functools

import jax
import jax.numpy as jnp
from jax import lax
from jax.experimental import pallas as pl
from jax.experimental.pallas import tpu as pltpu
from jax.sharding import PartitionSpec as P

norm_eps = 1e-06
group_size = 4
lanes = 128
MESH = pl.DeviceIdType.MESH


def shards_plain(tokens, norm_gain, gate_proj, up_proj, down_proj, expert_ids, route_weight):
    row_scale = norm_gain[None, :, None]
    gate_low = (gate_proj * row_scale).astype(jnp.bfloat16)
    up_low = (up_proj * row_scale).astype(jnp.bfloat16)
    down_low = down_proj.astype(jnp.bfloat16)
    width_fs = lax.axis_size("fs")
    width_tp = lax.axis_size("tp")

    def expand(matrix):
        return matrix.reshape((matrix.shape[0], 1) + matrix.shape[1:])

    def assemble(pieces):
        row_count, col_count = (pieces.shape[2], pieces.shape[3])
        tiled = pieces.reshape(width_fs, width_tp, row_count, col_count).transpose(0, 2, 1, 3)
        return tiled.reshape(1, width_fs * row_count, width_tp * col_count)

    arrived = (
        lax.all_to_all(expand(gate_low), ("fs", "tp"), split_axis=0, concat_axis=1, tiled=True),
        lax.all_to_all(expand(up_low), ("fs", "tp"), split_axis=0, concat_axis=1, tiled=True),
        lax.all_to_all(expand(down_low), ("fs", "tp"), split_axis=0, concat_axis=1, tiled=True),
    )
    new_gate, new_up, new_down = (assemble(arrived[0]), assemble(arrived[1]), assemble(arrived[2]))
    tok_count, width = tokens.shape
    experts = gate_proj.shape[0]
    slot_cap = 4 * tok_count // experts
    widened = tokens.astype(jnp.float32)
    normed = (
        widened * lax.rsqrt(jnp.mean(widened * widened, axis=-1, keepdims=True) + norm_eps)
    ).astype(jnp.bfloat16)
    flat_ids = expert_ids.reshape(-1)
    onehot = (flat_ids[:, None] == jnp.arange(experts, dtype=jnp.int32)[None, :]).astype(jnp.int32)
    slot_rank = jnp.sum(jnp.cumsum(onehot, axis=0) * onehot, axis=1) - 1
    slot_index = flat_ids * slot_cap + slot_rank
    source = (
        jnp.zeros((experts * slot_cap,), jnp.int32)
        .at[slot_index]
        .set(jnp.arange(2 * tok_count, dtype=jnp.int32) // 2 + 1)
    )
    filled = source > 0
    outgoing = jnp.where(
        filled[:, None], normed[jnp.maximum(source - 1, 0)], jnp.zeros((), jnp.bfloat16)
    )
    outgoing = outgoing.reshape(experts, slot_cap, width)
    arrived_rows = lax.all_to_all(outgoing, ("fs", "tp"), split_axis=0, concat_axis=0, tiled=True)
    flat_rows = arrived_rows.reshape(-1, width)
    gate_act = jnp.dot(flat_rows, new_gate[0], preferred_element_type=jnp.float32)
    up_act = jnp.dot(flat_rows, new_up[0], preferred_element_type=jnp.float32)
    hidden = (jax.nn.silu(gate_act) * up_act).astype(jnp.bfloat16)
    results = jnp.dot(hidden, new_down[0], preferred_element_type=jnp.float32).astype(jnp.bfloat16)
    returned = lax.all_to_all(
        results.reshape(arrived_rows.shape), ("fs", "tp"), split_axis=0, concat_axis=0, tiled=True
    )
    picked = returned.reshape(experts * slot_cap, width)[slot_index].reshape(tok_count, 2, width)
    mixed = jnp.sum(route_weight[:, :, None] * picked.astype(jnp.float32), axis=1).astype(
        jnp.bfloat16
    )
    return (mixed, new_gate, new_up, new_down)


def fused_kernel(
    n_fs, n_tp,
    x_in, ids_in, rw_in, gain_in, gate_in, up_in, down_in,
    gate_w, up_w, down_w, perm, fin_rx,
    x_ref, ids_ref, rw_ref, gain_ref,
    gate_st, up_st, down_st, gate_tx, up_tx, down_tx, early_st, early_tx,
    tok_tx, rows, wt_tx, wt_rx, wcol, hidden, own,
    part_tx, part_rx, sum_tx, sum_rx, fin_tx,
    in_sem, ld_sem, w_send, w_recv, tok_send, tok_recv, wt_send, wt_recv, ex_send, ex_recv,
    red_send, red_recv, y_send, y_recv, fin_send, fin_recv, early_sem, met_sem,
):
    f32, bf16 = jnp.float32, jnp.bfloat16
    fs, tp = lax.axis_index("fs"), lax.axis_index("tp")
    core = lax.rem(tp, 2)
    pair = tp // 2
    partner = tp + 1 - 2 * core
    across = lax.rem(tp + 2, n_tp)
    n_dev = n_fs * n_tp
    toks, width = x_ref.shape
    per = toks // n_fs
    d_rows, d_cols = down_in.shape[1:]
    chunks = d_cols // lanes
    srcs = (gate_in, up_in, down_in)
    stages = (gate_st, up_st, down_st)
    txs = (gate_tx, up_tx, down_tx)
    lands = (gate_w, up_w, down_w)

    quarter = n_fs // 4
    layer, col = fs // quarter, lax.rem(fs, quarter)
    plane = quarter * n_tp
    barrier = pltpu.get_barrier_semaphore()

    def greet_plane(sem):
        @pl.loop(1, plane)
        def _(k):
            at = lax.rem(col * n_tp + tp + k, plane)
            pl.semaphore_signal(
                sem, inc=1,
                device_id=(layer * quarter + at // n_tp, lax.rem(at, n_tp)),
                device_id_type=MESH,
            )

    for k in range(1, 4):
        pl.semaphore_signal(
            barrier, inc=1,
            device_id=(lax.rem(layer + k, 4) * quarter + col, tp), device_id_type=MESH,
        )
    greet_plane(barrier)
    half = layer // 2
    inner_far, outer_far, mate = 2 - half, 3 - 3 * half, 4 * half + 1 - layer

    def targets(layers):
        return [
            (at * quarter + lax.rem(col + 1 + i, quarter), at is layer and i == quarter - 1,
             i == quarter - 1 and at is not layer and at is not mate)
            for i in range(quarter)
            for at in layers
        ]

    far, close = targets((outer_far, inner_far)), targets((mate, layer))
    ahead = 1
    plan = far[:ahead] + close + far[ahead:]

    def load(m, tgt):
        at = pl.ds(tgt * n_tp, n_tp)
        return pltpu.make_async_copy(srcs[m].at[at], stages[m].at[at], ld_sem.at[m, tgt])

    small = [
        pltpu.make_async_copy(src, dst, in_sem.at[i])
        for i, (src, dst) in enumerate(
            ((gain_in, gain_ref), (x_in, x_ref), (ids_in, ids_ref), (rw_in, rw_ref))
        )
    ]
    early = [(m, j) for j in range(2) for m in (0, 1)]
    lines = (inner_far * quarter + col, outer_far * quarter + col)

    def load_early(m, j):
        return pltpu.make_async_copy(
            srcs[m].at[lines[j] * n_tp + tp], early_st.at[m, j], early_sem.at[m, j]
        )

    small[0].start()
    for m, j in early:
        load_early(m, j).start()
    for m in (0, 1):
        load(m, plan[0][0]).start()

    lane_id = lax.broadcasted_iota(jnp.int32, (toks, lanes), 1)
    row_id = lax.broadcasted_iota(jnp.int32, (toks, lanes), 0)
    in_group = lax.rem(row_id, per)
    span_lanes = group_size * per

    def as_columns(flat):
        spread_rows = jnp.concatenate([flat] * (8 // flat.shape[0]), axis=0)
        return jnp.transpose(spread_rows)

    def span(i):
        return pl.ds(pl.multiple_of(i * per, per), per)

    def all_sent(part, sem):
        pltpu.make_async_copy(part, part, sem).wait()

    def all_here(land, sem):
        pltpu.make_async_copy(land, land, sem).wait()

    small[0].wait()
    gain = jnp.broadcast_to(as_columns(gain_ref[...])[:, 0:1], gate_in.shape[1:])

    def cast(ms, tgt):
        for m in ms:
            load(m, tgt).wait()

            @pl.loop(0, n_tp)
            def _(t):
                block = stages[m][tgt * n_tp + t]
                if m < 2:
                    block = block * gain
                txs[m][tgt * n_tp + t] = block.astype(bf16)

    def block_at(m):
        r, c = srcs[m].shape[1:]
        return lands[m].at[pl.ds(pl.multiple_of(fs * r, r), r), pl.ds(pl.multiple_of(tp * c, c), c)]

    def send(tgt, same, begun):
        for t in range(1 if same or begun else 0, n_tp):
            to = lax.rem(tp + t, n_tp)
            for m in (0, 1):
                pltpu.make_async_remote_copy(
                    src_ref=txs[m].at[tgt * n_tp + to], dst_ref=block_at(m),
                    send_sem=w_send.at[m], recv_sem=w_recv.at[m],
                    device_id=(tgt, to), device_id_type=MESH,
                ).start()
        if same:
            for m in (0, 1):
                pltpu.make_async_copy(
                    txs[m].at[fs * n_tp + tp], block_at(m), w_recv.at[m]
                ).start()

    def step_plan(first, last):
        for k in range(first, last):
            if k < len(plan):
                cast((0, 1), plan[k][0])
            if k > 0:
                send(*plan[k - 1])

    def chunk_block(k):
        return down_w.at[
            pl.ds(pl.multiple_of(fs * d_rows, d_rows), d_rows),
            pl.ds(pl.multiple_of(tp * d_cols + k * lanes, lanes), lanes),
        ]

    def send_chunk(k):
        for tgt, same, _ in close + far:
            for t in range(1 if same else 0, n_tp):
                to = lax.rem(tp + t, n_tp)
                pltpu.make_async_remote_copy(
                    src_ref=down_tx.at[tgt * n_tp + to, :, pl.ds(k * lanes, lanes)],
                    dst_ref=chunk_block(k),
                    send_sem=w_send.at[2 + k], recv_sem=w_recv.at[2 + k],
                    device_id=(tgt, to), device_id_type=MESH,
                ).start()
            if same:
                pltpu.make_async_copy(
                    down_tx.at[fs * n_tp + tp, :, pl.ds(k * lanes, lanes)],
                    chunk_block(k), w_recv.at[2 + k],
                ).start()

    for m, j in early:
        load_early(m, j).wait()
        early_tx[m, j] = (early_st[m, j] * gain).astype(bf16)
    pl.semaphore_wait(barrier, plane + 2)
    greet_plane(met_sem)
    for m, j in early:
        pltpu.make_async_remote_copy(
            src_ref=early_tx.at[m, j], dst_ref=block_at(m),
            send_sem=w_send.at[m], recv_sem=w_recv.at[m],
            device_id=(lines[j], tp), device_id_type=MESH,
        ).start()
    step_plan(0, 1)
    for copy in small[1:]:
        copy.start()
    for ms in ((0, 1), (2,)):
        for tgt, _, _ in plan[1:] if ms[0] == 0 else plan:
            for m in ms:
                load(m, tgt).start()
    pl.semaphore_wait(met_sem, plane - 1)
    step_plan(1, ahead + 1)

    for copy in small[1:]:
        copy.wait()
    x = x_ref[...].astype(f32)
    scale = lax.rsqrt(jnp.mean(x * x, axis=-1, keepdims=True) + norm_eps)
    normed = (x * scale).astype(bf16)
    idf = as_columns(ids_ref[...].astype(f32))
    grp = jnp.floor((idf + 0.5) * (1.0 / group_size))
    slot = lax.broadcasted_iota(jnp.int32, (toks, toks), 1).astype(f32)
    tok = lax.broadcasted_iota(jnp.int32, (toks, toks), 0).astype(f32)
    slot_grp = jnp.floor((slot + 0.5) * (1.0 / per))
    named = (grp[:, 0:1] == slot_grp).astype(f32)
    before = (slot < tok).astype(f32)
    rank = jnp.dot(before.astype(bf16), named.astype(bf16), preferred_element_type=f32)
    place = jnp.where(rank == slot - slot_grp * per, named, 0.0).astype(bf16)
    perm[...] = place
    by_slot = (((0,), (0,)), ((), ()))
    tok_tx[...] = lax.dot_general(
        place, normed, by_slot, preferred_element_type=f32
    ).astype(bf16)

    @pl.loop(1, n_fs)
    def _(j):
        tgt = lax.rem(fs + j, n_fs)
        pltpu.make_async_remote_copy(
            src_ref=tok_tx.at[span(tgt)], dst_ref=rows.at[tp, span(fs)],
            send_sem=tok_send, recv_sem=tok_recv,
            device_id=(tgt, tp), device_id_type=MESH,
        ).start()

    pltpu.make_async_copy(tok_tx.at[span(fs)], rows.at[tp, span(fs)], tok_recv).start()

    lane_pick = (lax.rem(lane_id, span_lanes) // per).astype(f32)
    local = idf - grp * group_size
    rw = as_columns(rw_ref[...])
    wv = jnp.where(local[:, 0:1] == lane_pick, rw[:, 0:1], 0.0) + jnp.where(
        local[:, 1:2] == lane_pick, rw[:, 1:2], 0.0
    )
    high = wv.astype(bf16).astype(f32)
    aug = jnp.where(lane_id < span_lanes, high, wv - high).astype(bf16)
    by_row = lax.dot_general(place, aug, by_slot, preferred_element_type=f32)
    by_row = jnp.where(lax.rem(lane_id, per) == in_group, by_row, 0.0)
    wt_tx[...] = jnp.sum(by_row.reshape(n_fs, per, lanes), axis=1, keepdims=True)

    @pl.loop(1, n_dev)
    def _(k):
        dev = lax.rem(fs * n_tp + tp + k, n_dev)
        tgt = dev // n_tp
        pltpu.make_async_remote_copy(
            src_ref=wt_tx.at[tgt], dst_ref=wt_rx.at[tp, fs],
            send_sem=wt_send, recv_sem=wt_recv,
            device_id=(tgt, lax.rem(dev, n_tp)), device_id_type=MESH,
        ).start()

    pltpu.make_async_copy(wt_tx.at[fs], wt_rx.at[tp, fs], wt_recv).start()

    step_plan(ahead + 1, len(plan) + 1)
    for tgt, _, _ in plan:
        cast((2,), tgt)
    for k in range(chunks):
        send_chunk(k)

    def swap(src, dst, to, send_sem, recv_sem):
        return pltpu.make_async_remote_copy(
            src_ref=src, dst_ref=dst, send_sem=send_sem, recv_sem=recv_sem,
            device_id=(fs, to), device_id_type=MESH,
        )

    all_here(rows.at[tp], tok_recv)
    cross = swap(rows.at[tp], rows.at[tp], across, ex_send.at[0], ex_recv.at[0])
    cross.start()
    near = swap(rows.at[tp], rows.at[tp], partner, ex_send.at[1], ex_recv.at[1])
    near.start()
    cross.wait()
    other = swap(rows.at[across], rows.at[across], partner, ex_send.at[2], ex_recv.at[2])
    other.start()
    near.wait()
    other.wait()
    all_here(wt_rx, wt_recv)
    mine = lax.rem(lane_id, span_lanes) == tp * per + in_group

    @pl.loop(0, n_tp)
    def _(q):
        w = jnp.broadcast_to(wt_rx[q], (n_fs, per, lanes)).reshape(toks, lanes)
        wcol[q] = jnp.broadcast_to(
            jnp.sum(jnp.where(mine, w, 0.0), axis=-1, keepdims=True), (toks, lanes)
        )

    for m in (0, 1):
        all_here(lands[m], w_recv.at[m])

    @pl.loop(0, n_tp)
    def _(q):
        g = jnp.dot(rows[q], gate_w[...], preferred_element_type=f32)
        u = jnp.dot(rows[q], up_w[...], preferred_element_type=f32)
        hidden[q] = (g / (1.0 + jnp.exp(-g)) * u).astype(bf16)

    pieces = 4
    step = n_fs // pieces

    def piece(p):
        return lax.rem(half * 2 + 2 + p, pieces)

    def piece_rows(p):
        return pl.ds(pl.multiple_of(piece(p) * step * per, step * per), step * per)

    def reduce_near(k):
        return swap(part_tx.at[k], part_rx.at[k], partner, red_send.at[k], red_recv.at[k])

    def over(k, p):
        at = piece_rows(p)
        return swap(
            sum_tx.at[k, at], sum_rx.at[k, at], across, y_send.at[k, p], y_recv.at[k, p]
        )

    def multiply(k):
        columns = jnp.concatenate(
            [down_w[:, pl.ds(t * d_cols + k * lanes, lanes)] for t in range(n_tp)], axis=1
        )

        def partial(q):
            w = jnp.concatenate([wcol[q]] * n_tp, axis=1)
            return jnp.dot(hidden[q], columns, preferred_element_type=f32) * w

        for side in range(2):
            part_tx[k, side] = partial(side * 2 + 1 - core).astype(bf16)
        reduce_near(k).start()
        own[k, 0] = partial((1 - pair) * 2 + core)
        own[k, 1] = partial(pair * 2 + core)

    def cross_over(k):
        reduce_near(k).wait()
        for p in range(pieces):
            at = piece_rows(p)
            sum_tx[k, at] = (own[k, 0, at] + part_rx[k, 1 - pair, at].astype(f32)).astype(bf16)
            over(k, p).start()

    def give_back(k):
        for p in range(pieces):
            at = piece_rows(p)
            own_part = own[k, 1, at] + part_rx[k, pair, at].astype(f32)
            over(k, p).wait()
            fin_tx[k, at] = (own_part + sum_rx[k, at].astype(f32)).astype(bf16)
            for i in range(step):
                to = piece(p) * step + i

                @pl.when(to != fs)
                def _():
                    pltpu.make_async_remote_copy(
                        src_ref=fin_tx.at[k, span(to)], dst_ref=fin_rx.at[k, span(fs)],
                        send_sem=fin_send, recv_sem=fin_recv,
                        device_id=(to, tp), device_id_type=MESH,
                    ).start()

                @pl.when(to == fs)
                def _():
                    pltpu.make_async_copy(
                        fin_tx.at[k, span(fs)], fin_rx.at[k, span(fs)], fin_recv
                    ).start()

    chunk_area = down_w.at[:, pl.ds(0, n_tp * lanes)]
    for k in range(chunks):
        all_here(chunk_area, w_recv.at[2 + k])
        multiply(k)
        if k > 1:
            give_back(k - 2)
        cross_over(k)
    give_back(chunks - 2)
    give_back(chunks - 1)

    for m in (0, 1):
        all_sent(txs[m].at[pl.ds(0, n_dev - 1)], w_send.at[m])
    for k in range(chunks):
        all_sent(down_tx.at[pl.ds(0, n_dev - 1), :, pl.ds(0, lanes)], w_send.at[2 + k])
    all_sent(tok_tx.at[pl.ds(0, toks - per)], tok_send)
    all_sent(wt_rx.at[0, pl.ds(0, n_fs - 1)], wt_send)
    for _ in range(n_tp - 1):
        all_sent(wt_rx.at[0], wt_send)
    all_sent(fin_tx.at[:, pl.ds(0, toks - per)], fin_send)
    all_here(fin_rx, fin_recv)


def write_kernel(perm, fin_rx, gate, up, down, mixed_out, gate_out, up_out, down_out, mixed, sem):
    chunks, _, wide = fin_rx.shape
    blocks = wide // lanes
    moves = ((gate, gate_out), (up, up_out), (down, down_out), (mixed, mixed_out))

    def put(m):
        return pltpu.make_async_copy(moves[m][0], moves[m][1], sem.at[m])

    for m in range(3):
        put(m).start()
    for k in range(chunks):
        part = jnp.dot(
            perm[...], fin_rx[k], preferred_element_type=jnp.float32
        ).astype(jnp.bfloat16)
        for t in range(blocks):
            mixed[:, pl.ds((t * chunks + k) * lanes, lanes)] = part[:, t * lanes:(t + 1) * lanes]
    put(3).start()
    for m in range(4):
        put(m).wait()


def shards_fused(n_fs, n_tp, tokens, norm_gain, gate_proj, up_proj, down_proj, expert_ids, route_weight):
    f32, bf16 = jnp.float32, jnp.bfloat16
    n_dev = n_fs * n_tp
    toks, width = tokens.shape
    _, gr, gc = gate_proj.shape
    _, dr, dc = down_proj.shape
    inner = gc * n_tp
    chunks, wide = dc // lanes, n_tp * lanes
    vmem = pl.BlockSpec(memory_space=pltpu.VMEM)
    hbm = pl.BlockSpec(memory_space=pltpu.HBM)
    dma = pltpu.SemaphoreType.DMA
    new_gate, new_up, new_down, perm, returned = pl.pallas_call(
        functools.partial(fused_kernel, n_fs, n_tp),
        out_shape=(
            pltpu.VMEM((width, inner), bf16),
            pltpu.VMEM((width, inner), bf16),
            pltpu.VMEM((inner, width), bf16),
            pltpu.VMEM((toks, toks), bf16),
            pltpu.VMEM((chunks, toks, wide), bf16),
        ),
        in_specs=[hbm] * 7,
        out_specs=(vmem,) * 5,
        scratch_shapes=[
            pltpu.VMEM(tokens.shape, bf16),
            pltpu.VMEM((2, toks), jnp.int32),
            pltpu.VMEM((2, toks), f32),
            pltpu.VMEM((1, gr), f32),
            pltpu.VMEM((n_dev, gr, gc), f32),
            pltpu.VMEM((n_dev, gr, gc), f32),
            pltpu.VMEM((n_dev, dr, dc), f32),
            pltpu.VMEM((n_dev, gr, gc), bf16),
            pltpu.VMEM((n_dev, gr, gc), bf16),
            pltpu.VMEM((n_dev, dr, dc), bf16),
            pltpu.VMEM((2, 2, gr, gc), f32),
            pltpu.VMEM((2, 2, gr, gc), bf16),
            pltpu.VMEM((toks, width), bf16),
            pltpu.VMEM((n_tp, toks, width), bf16),
            pltpu.VMEM((n_fs, 1, lanes), f32),
            pltpu.VMEM((n_tp, n_fs, 1, lanes), f32),
            pltpu.VMEM((n_tp, toks, lanes), f32),
            pltpu.VMEM((n_tp, toks, inner), bf16),
            pltpu.VMEM((chunks, 2, toks, wide), f32),
            pltpu.VMEM((chunks, 2, toks, wide), bf16),
            pltpu.VMEM((chunks, 2, toks, wide), bf16),
            pltpu.VMEM((chunks, toks, wide), bf16),
            pltpu.VMEM((chunks, toks, wide), bf16),
            pltpu.VMEM((chunks, toks, wide), bf16),
            dma((4,)), dma((3, n_fs)), dma((2 + chunks,)), dma((2 + chunks,)), dma, dma, dma, dma,
            dma((3,)), dma((3,)), dma((chunks,)), dma((chunks,)), dma((chunks, 4)),
            dma((chunks, 4)), dma, dma, dma((2, 2)), pltpu.SemaphoreType.REGULAR,
        ],
        compiler_params=pltpu.CompilerParams(
            collective_id=0, has_side_effects=True, vmem_limit_bytes=47 * 1024 * 1024
        ),
    )(*(
        pltpu.with_memory_space_constraint(a, pltpu.HBM)
        for a in (
            tokens, expert_ids.T, route_weight.T, norm_gain[None, :], gate_proj, up_proj, down_proj
        )
    ))
    mixed, new_gate, new_up, new_down = pl.pallas_call(
        write_kernel,
        out_shape=(
            jax.ShapeDtypeStruct((toks, width), bf16),
            jax.ShapeDtypeStruct((width, inner), bf16),
            jax.ShapeDtypeStruct((width, inner), bf16),
            jax.ShapeDtypeStruct((inner, width), bf16),
        ),
        in_specs=[vmem] * 5,
        out_specs=(hbm,) * 4,
        scratch_shapes=[pltpu.VMEM((toks, width), bf16), dma((4,))],
        compiler_params=pltpu.CompilerParams(vmem_limit_bytes=16 * 1024 * 1024),
    )(perm, returned, new_gate, new_up, new_down)
    return mixed, new_gate[None], new_up[None], new_down[None]


def shards(n_fs, n_tp, *args):
    tokens, _, gate_proj, _, down_proj = args[:5]
    toks, experts = tokens.shape[0], gate_proj.shape[0]
    whole_tiles = (
        n_tp == group_size
        and experts == n_fs * n_tp
        and toks % (16 * n_fs) == 0
        and n_fs % 4 == 0
        and gate_proj.shape[2] % 128 == 0
        and down_proj.shape[2] % 128 == 0
        and gate_proj.shape[1] % 16 == 0
        and down_proj.shape[1] % 16 == 0
        and 2 * group_size * toks == lanes * n_fs
    )
    if whole_tiles:
        return shards_fused(n_fs, n_tp, *args)
    return shards_plain(*args)


def solution(mesh):
    in_specs = (
        P(("fs", "tp"), None),
        P("fs"),
        P(None, "fs", "tp"),
        P(None, "fs", "tp"),
        P(None, "fs", "tp"),
        P(("fs", "tp"), None),
        P(("fs", "tp"), None),
    )
    out_specs = (
        P(("fs", "tp"), None),
        P(("fs", "tp"), None, None),
        P(("fs", "tp"), None, None),
        P(("fs", "tp"), None, None),
    )
    body = functools.partial(shards, mesh.shape["fs"], mesh.shape["tp"])
    return jax.shard_map(body, mesh=mesh, in_specs=in_specs, out_specs=out_specs, check_vma=False)
```

```python
import functools

import jax
import jax.numpy as jnp
from jax import lax
from jax.experimental import pallas as pl
from jax.experimental.pallas import tpu as pltpu
from jax.sharding import PartitionSpec as P

norm_eps = 1e-06
group_size = 4
lanes = 128
last_cuts = 2
MESH = pl.DeviceIdType.MESH


def shards_plain(tokens, norm_gain, gate_proj, up_proj, down_proj, expert_ids, route_weight):
    row_scale = norm_gain[None, :, None]
    gate_low = (gate_proj * row_scale).astype(jnp.bfloat16)
    up_low = (up_proj * row_scale).astype(jnp.bfloat16)
    down_low = down_proj.astype(jnp.bfloat16)
    width_fs = lax.axis_size("fs")
    width_tp = lax.axis_size("tp")

    def expand(matrix):
        return matrix.reshape((matrix.shape[0], 1) + matrix.shape[1:])

    def assemble(pieces):
        row_count, col_count = (pieces.shape[2], pieces.shape[3])
        tiled = pieces.reshape(width_fs, width_tp, row_count, col_count).transpose(0, 2, 1, 3)
        return tiled.reshape(1, width_fs * row_count, width_tp * col_count)

    arrived = (
        lax.all_to_all(expand(gate_low), ("fs", "tp"), split_axis=0, concat_axis=1, tiled=True),
        lax.all_to_all(expand(up_low), ("fs", "tp"), split_axis=0, concat_axis=1, tiled=True),
        lax.all_to_all(expand(down_low), ("fs", "tp"), split_axis=0, concat_axis=1, tiled=True),
    )
    new_gate, new_up, new_down = (assemble(arrived[0]), assemble(arrived[1]), assemble(arrived[2]))
    tok_count, width = tokens.shape
    experts = gate_proj.shape[0]
    slot_cap = 4 * tok_count // experts
    widened = tokens.astype(jnp.float32)
    normed = (
        widened * lax.rsqrt(jnp.mean(widened * widened, axis=-1, keepdims=True) + norm_eps)
    ).astype(jnp.bfloat16)
    flat_ids = expert_ids.reshape(-1)
    onehot = (flat_ids[:, None] == jnp.arange(experts, dtype=jnp.int32)[None, :]).astype(jnp.int32)
    slot_rank = jnp.sum(jnp.cumsum(onehot, axis=0) * onehot, axis=1) - 1
    slot_index = flat_ids * slot_cap + slot_rank
    source = (
        jnp.zeros((experts * slot_cap,), jnp.int32)
        .at[slot_index]
        .set(jnp.arange(2 * tok_count, dtype=jnp.int32) // 2 + 1)
    )
    filled = source > 0
    outgoing = jnp.where(
        filled[:, None], normed[jnp.maximum(source - 1, 0)], jnp.zeros((), jnp.bfloat16)
    )
    outgoing = outgoing.reshape(experts, slot_cap, width)
    arrived_rows = lax.all_to_all(outgoing, ("fs", "tp"), split_axis=0, concat_axis=0, tiled=True)
    flat_rows = arrived_rows.reshape(-1, width)
    gate_act = jnp.dot(flat_rows, new_gate[0], preferred_element_type=jnp.float32)
    up_act = jnp.dot(flat_rows, new_up[0], preferred_element_type=jnp.float32)
    hidden = (jax.nn.silu(gate_act) * up_act).astype(jnp.bfloat16)
    results = jnp.dot(hidden, new_down[0], preferred_element_type=jnp.float32).astype(jnp.bfloat16)
    returned = lax.all_to_all(
        results.reshape(arrived_rows.shape), ("fs", "tp"), split_axis=0, concat_axis=0, tiled=True
    )
    picked = returned.reshape(experts * slot_cap, width)[slot_index].reshape(tok_count, 2, width)
    mixed = jnp.sum(route_weight[:, :, None] * picked.astype(jnp.float32), axis=1).astype(
        jnp.bfloat16
    )
    return (mixed, new_gate, new_up, new_down)


def fused_kernel(
    n_fs, n_tp,
    x_in, ids_in, rw_in, gain_in, gate_in, up_in, down_in,
    gate_w, up_w, down_w, perm, fin_rx,
    x_ref, ids_ref, rw_ref, gain_ref,
    gate_st, up_st, down_st, gate_tx, up_tx, down_tx, early_st, early_tx,
    tok_tx, rows, wt_tx, wt_rx, wcol, hidden, own,
    part_tx, part_rx, sum_tx, sum_rx, fin_tx,
    in_sem, ld_sem, w_send, w_recv, tok_send, tok_recv, wt_send, wt_recv, ex_send, ex_recv,
    red_send, red_recv, y_send, y_recv, fin_send, fin_recv, early_sem, met_sem,
):
    f32, bf16 = jnp.float32, jnp.bfloat16
    fs, tp = lax.axis_index("fs"), lax.axis_index("tp")
    core = lax.rem(tp, 2)
    pair = tp // 2
    partner = tp + 1 - 2 * core
    across = lax.rem(tp + 2, n_tp)
    n_dev = n_fs * n_tp
    toks, width = x_ref.shape
    per = toks // n_fs
    d_rows, d_cols = down_in.shape[1:]
    chunks = d_cols // lanes
    srcs = (gate_in, up_in, down_in)
    stages = (gate_st, up_st, down_st)
    txs = (gate_tx, up_tx, down_tx)
    lands = (gate_w, up_w, down_w)

    quarter = n_fs // 4
    layer, col = fs // quarter, lax.rem(fs, quarter)
    plane = quarter * n_tp
    barrier = pltpu.get_barrier_semaphore()

    def greet_plane(sem):
        @pl.loop(1, plane)
        def _(k):
            at = lax.rem(col * n_tp + tp + k, plane)
            pl.semaphore_signal(
                sem, inc=1,
                device_id=(layer * quarter + at // n_tp, lax.rem(at, n_tp)),
                device_id_type=MESH,
            )

    for k in range(1, 4):
        pl.semaphore_signal(
            barrier, inc=1,
            device_id=(lax.rem(layer + k, 4) * quarter + col, tp), device_id_type=MESH,
        )
    greet_plane(barrier)
    half = layer // 2
    inner_far, outer_far, mate = 2 - half, 3 - 3 * half, 4 * half + 1 - layer

    def targets(layers):
        return [
            (at * quarter + lax.rem(col + 1 + i, quarter), at is layer and i == quarter - 1,
             i == quarter - 1 and at is not layer and at is not mate)
            for i in range(quarter)
            for at in layers
        ]

    far, close = targets((outer_far, inner_far)), targets((mate, layer))
    ahead = 1
    plan = far[:ahead] + close + far[ahead:]

    def load(m, tgt):
        at = pl.ds(tgt * n_tp, n_tp)
        return pltpu.make_async_copy(srcs[m].at[at], stages[m].at[at], ld_sem.at[m, tgt])

    small = [
        pltpu.make_async_copy(src, dst, in_sem.at[i])
        for i, (src, dst) in enumerate(
            ((gain_in, gain_ref), (x_in, x_ref), (ids_in, ids_ref), (rw_in, rw_ref))
        )
    ]
    early = [(m, j) for j in range(2) for m in (0, 1)]
    lines = (inner_far * quarter + col, outer_far * quarter + col)

    def load_early(m, j):
        return pltpu.make_async_copy(
            srcs[m].at[lines[j] * n_tp + tp], early_st.at[m, j], early_sem.at[m, j]
        )

    small[0].start()
    for m, j in early:
        load_early(m, j).start()
    for m in (0, 1):
        load(m, plan[0][0]).start()

    lane_id = lax.broadcasted_iota(jnp.int32, (toks, lanes), 1)
    row_id = lax.broadcasted_iota(jnp.int32, (toks, lanes), 0)
    in_group = lax.rem(row_id, per)
    span_lanes = group_size * per

    def as_columns(flat):
        spread_rows = jnp.concatenate([flat] * (8 // flat.shape[0]), axis=0)
        return jnp.transpose(spread_rows)

    def span(i):
        return pl.ds(pl.multiple_of(i * per, per), per)

    def all_sent(part, sem):
        pltpu.make_async_copy(part, part, sem).wait()

    def all_here(land, sem):
        pltpu.make_async_copy(land, land, sem).wait()

    small[0].wait()
    gain = jnp.broadcast_to(as_columns(gain_ref[...])[:, 0:1], gate_in.shape[1:])

    def cast(ms, tgt):
        for m in ms:
            load(m, tgt).wait()

            @pl.loop(0, n_tp)
            def _(t):
                block = stages[m][tgt * n_tp + t]
                if m < 2:
                    block = block * gain
                txs[m][tgt * n_tp + t] = block.astype(bf16)

    def block_at(m):
        r, c = srcs[m].shape[1:]
        return lands[m].at[pl.ds(pl.multiple_of(fs * r, r), r), pl.ds(pl.multiple_of(tp * c, c), c)]

    def send(tgt, same, begun):
        for t in range(1 if same or begun else 0, n_tp):
            to = lax.rem(tp + t, n_tp)
            for m in (0, 1):
                pltpu.make_async_remote_copy(
                    src_ref=txs[m].at[tgt * n_tp + to], dst_ref=block_at(m),
                    send_sem=w_send.at[m], recv_sem=w_recv.at[m],
                    device_id=(tgt, to), device_id_type=MESH,
                ).start()
        if same:
            for m in (0, 1):
                pltpu.make_async_copy(
                    txs[m].at[fs * n_tp + tp], block_at(m), w_recv.at[m]
                ).start()

    def step_plan(first, last):
        for k in range(first, last):
            if k < len(plan):
                cast((0, 1), plan[k][0])
            if k > 0:
                send(*plan[k - 1])

    cuts = [(k, 0, d_rows) for k in range(chunks - 1)]
    cuts += [(chunks - 1, i * d_rows // last_cuts, d_rows // last_cuts) for i in range(last_cuts)]

    def send_cut(c):
        k, row, count = cuts[c]
        piece_of = (pl.ds(row, count), pl.ds(k * lanes, lanes))
        land = down_w.at[
            pl.ds(pl.multiple_of(fs * d_rows + row, count), count),
            pl.ds(pl.multiple_of(tp * d_cols + k * lanes, lanes), lanes),
        ]
        for tgt, same, _ in close + far:
            for t in range(1 if same else 0, n_tp):
                to = lax.rem(tp + t, n_tp)
                pltpu.make_async_remote_copy(
                    src_ref=down_tx.at[(tgt * n_tp + to,) + piece_of], dst_ref=land,
                    send_sem=w_send.at[2 + c], recv_sem=w_recv.at[2 + c],
                    device_id=(tgt, to), device_id_type=MESH,
                ).start()
            if same:
                pltpu.make_async_copy(
                    down_tx.at[(fs * n_tp + tp,) + piece_of], land, w_recv.at[2 + c]
                ).start()

    for m, j in early:
        load_early(m, j).wait()
        early_tx[m, j] = (early_st[m, j] * gain).astype(bf16)
    pl.semaphore_wait(barrier, plane + 2)
    greet_plane(met_sem)
    for m, j in early:
        pltpu.make_async_remote_copy(
            src_ref=early_tx.at[m, j], dst_ref=block_at(m),
            send_sem=w_send.at[m], recv_sem=w_recv.at[m],
            device_id=(lines[j], tp), device_id_type=MESH,
        ).start()
    step_plan(0, 1)
    for copy in small[1:]:
        copy.start()
    for ms in ((0, 1), (2,)):
        for tgt, _, _ in plan[1:] if ms[0] == 0 else plan:
            for m in ms:
                load(m, tgt).start()
    pl.semaphore_wait(met_sem, plane - 1)
    step_plan(1, ahead + 1)

    for copy in small[1:]:
        copy.wait()
    x = x_ref[...].astype(f32)
    scale = lax.rsqrt(jnp.mean(x * x, axis=-1, keepdims=True) + norm_eps)
    normed = (x * scale).astype(bf16)
    idf = as_columns(ids_ref[...].astype(f32))
    grp = jnp.floor((idf + 0.5) * (1.0 / group_size))
    slot = lax.broadcasted_iota(jnp.int32, (toks, toks), 1).astype(f32)
    tok = lax.broadcasted_iota(jnp.int32, (toks, toks), 0).astype(f32)
    slot_grp = jnp.floor((slot + 0.5) * (1.0 / per))
    named = (grp[:, 0:1] == slot_grp).astype(f32)
    before = (slot < tok).astype(f32)
    rank = jnp.dot(before.astype(bf16), named.astype(bf16), preferred_element_type=f32)
    place = jnp.where(rank == slot - slot_grp * per, named, 0.0).astype(bf16)
    perm[...] = place
    by_slot = (((0,), (0,)), ((), ()))
    tok_tx[...] = lax.dot_general(
        place, normed, by_slot, preferred_element_type=f32
    ).astype(bf16)

    @pl.loop(1, n_fs)
    def _(j):
        tgt = lax.rem(fs + j, n_fs)
        pltpu.make_async_remote_copy(
            src_ref=tok_tx.at[span(tgt)], dst_ref=rows.at[tp, span(fs)],
            send_sem=tok_send, recv_sem=tok_recv,
            device_id=(tgt, tp), device_id_type=MESH,
        ).start()

    pltpu.make_async_copy(tok_tx.at[span(fs)], rows.at[tp, span(fs)], tok_recv).start()

    lane_pick = (lax.rem(lane_id, span_lanes) // per).astype(f32)
    local = idf - grp * group_size
    rw = as_columns(rw_ref[...])
    wv = jnp.where(local[:, 0:1] == lane_pick, rw[:, 0:1], 0.0) + jnp.where(
        local[:, 1:2] == lane_pick, rw[:, 1:2], 0.0
    )
    high = wv.astype(bf16).astype(f32)
    aug = jnp.where(lane_id < span_lanes, high, wv - high).astype(bf16)
    by_row = lax.dot_general(place, aug, by_slot, preferred_element_type=f32)
    by_row = jnp.where(lax.rem(lane_id, per) == in_group, by_row, 0.0)
    wt_tx[...] = jnp.sum(by_row.reshape(n_fs, per, lanes), axis=1, keepdims=True)

    @pl.loop(1, n_dev)
    def _(k):
        dev = lax.rem(fs * n_tp + tp + k, n_dev)
        tgt = dev // n_tp
        pltpu.make_async_remote_copy(
            src_ref=wt_tx.at[tgt], dst_ref=wt_rx.at[tp, fs],
            send_sem=wt_send, recv_sem=wt_recv,
            device_id=(tgt, lax.rem(dev, n_tp)), device_id_type=MESH,
        ).start()

    pltpu.make_async_copy(wt_tx.at[fs], wt_rx.at[tp, fs], wt_recv).start()

    step_plan(ahead + 1, len(plan) + 1)
    for tgt, _, _ in plan:
        cast((2,), tgt)
    for c in range(len(cuts)):
        send_cut(c)

    def swap(src, dst, to, send_sem, recv_sem):
        return pltpu.make_async_remote_copy(
            src_ref=src, dst_ref=dst, send_sem=send_sem, recv_sem=recv_sem,
            device_id=(fs, to), device_id_type=MESH,
        )

    all_here(rows.at[tp], tok_recv)
    cross = swap(rows.at[tp], rows.at[tp], across, ex_send.at[0], ex_recv.at[0])
    cross.start()
    near = swap(rows.at[tp], rows.at[tp], partner, ex_send.at[1], ex_recv.at[1])
    near.start()
    cross.wait()
    other = swap(rows.at[across], rows.at[across], partner, ex_send.at[2], ex_recv.at[2])
    other.start()
    near.wait()
    other.wait()
    all_here(wt_rx, wt_recv)
    mine = lax.rem(lane_id, span_lanes) == tp * per + in_group

    @pl.loop(0, n_tp)
    def _(q):
        w = jnp.broadcast_to(wt_rx[q], (n_fs, per, lanes)).reshape(toks, lanes)
        wcol[q] = jnp.broadcast_to(
            jnp.sum(jnp.where(mine, w, 0.0), axis=-1, keepdims=True), (toks, lanes)
        )

    for m in (0, 1):
        all_here(lands[m], w_recv.at[m])

    @pl.loop(0, n_tp)
    def _(q):
        g = jnp.dot(rows[q], gate_w[...], preferred_element_type=f32)
        u = jnp.dot(rows[q], up_w[...], preferred_element_type=f32)
        hidden[q] = (g / (1.0 + jnp.exp(-g)) * u).astype(bf16)

    pieces = 4
    step = n_fs // pieces

    def piece(p):
        return lax.rem(half * 2 + 2 + p, pieces)

    def piece_rows(p):
        return pl.ds(pl.multiple_of(piece(p) * step * per, step * per), step * per)

    def reduce_near(k):
        return swap(part_tx.at[k], part_rx.at[k], partner, red_send.at[k], red_recv.at[k])

    def over(k, p):
        at = piece_rows(p)
        return swap(
            sum_tx.at[k, at], sum_rx.at[k, at], across, y_send.at[k, p], y_recv.at[k, p]
        )

    def multiply(k):
        columns = jnp.concatenate(
            [down_w[:, pl.ds(t * d_cols + k * lanes, lanes)] for t in range(n_tp)], axis=1
        )

        def partial(q):
            w = jnp.concatenate([wcol[q]] * n_tp, axis=1)
            return jnp.dot(hidden[q], columns, preferred_element_type=f32) * w

        for side in range(2):
            part_tx[k, side] = partial(side * 2 + 1 - core).astype(bf16)
        reduce_near(k).start()
        own[k, 0] = partial((1 - pair) * 2 + core)
        own[k, 1] = partial(pair * 2 + core)

    def cross_over(k):
        reduce_near(k).wait()
        for p in range(pieces):
            at = piece_rows(p)
            sum_tx[k, at] = (own[k, 0, at] + part_rx[k, 1 - pair, at].astype(f32)).astype(bf16)
            over(k, p).start()

    def give_back(k, ps=tuple(range(4))):
        for p in ps:
            at = piece_rows(p)
            own_part = own[k, 1, at] + part_rx[k, pair, at].astype(f32)
            over(k, p).wait()
            fin_tx[k, at] = (own_part + sum_rx[k, at].astype(f32)).astype(bf16)
            for i in range(step):
                to = piece(p) * step + i

                @pl.when(to != fs)
                def _():
                    pltpu.make_async_remote_copy(
                        src_ref=fin_tx.at[k, span(to)], dst_ref=fin_rx.at[k, span(fs)],
                        send_sem=fin_send, recv_sem=fin_recv,
                        device_id=(to, tp), device_id_type=MESH,
                    ).start()

                @pl.when(to == fs)
                def _():
                    pltpu.make_async_copy(
                        fin_tx.at[k, span(fs)], fin_rx.at[k, span(fs)], fin_recv
                    ).start()

    def cut_here(c):
        area = down_w.at[pl.ds(0, n_fs * cuts[c][2]), pl.ds(0, n_tp * lanes)]
        all_here(area, w_recv.at[2 + c])

    for k in range(chunks - 1):
        cut_here(k)
        multiply(k)
        cross_over(k)
    last = chunks - 1
    cut_here(last)
    give_back(0)
    give_back(1, (0,))
    cut_here(last + 1)
    multiply(last)
    cross_over(last)
    give_back(last - 1, (0,))
    give_back(last, (0,))
    for k in range(1, chunks):
        give_back(k, (1, 2, 3))

    for m in (0, 1):
        all_sent(txs[m].at[pl.ds(0, n_dev - 1)], w_send.at[m])
    for c, (_, _, count) in enumerate(cuts):
        all_sent(
            down_tx.at[pl.ds(0, n_dev - 1), pl.ds(0, count), pl.ds(0, lanes)], w_send.at[2 + c]
        )
    all_sent(tok_tx.at[pl.ds(0, toks - per)], tok_send)
    all_sent(wt_rx.at[0, pl.ds(0, n_fs - 1)], wt_send)
    for _ in range(n_tp - 1):
        all_sent(wt_rx.at[0], wt_send)
    all_sent(fin_tx.at[:, pl.ds(0, toks - per)], fin_send)
    all_here(fin_rx, fin_recv)


def write_kernel(perm, fin_rx, gate, up, down, mixed_out, gate_out, up_out, down_out, mixed, sem):
    chunks, _, wide = fin_rx.shape
    blocks = wide // lanes
    moves = ((gate, gate_out), (up, up_out), (down, down_out), (mixed, mixed_out))

    def put(m):
        return pltpu.make_async_copy(moves[m][0], moves[m][1], sem.at[m])

    for m in range(3):
        put(m).start()
    for k in range(chunks):
        part = jnp.dot(
            perm[...], fin_rx[k], preferred_element_type=jnp.float32
        ).astype(jnp.bfloat16)
        for t in range(blocks):
            mixed[:, pl.ds((t * chunks + k) * lanes, lanes)] = part[:, t * lanes:(t + 1) * lanes]
    put(3).start()
    for m in range(4):
        put(m).wait()


def shards_fused(n_fs, n_tp, tokens, norm_gain, gate_proj, up_proj, down_proj, expert_ids, route_weight):
    f32, bf16 = jnp.float32, jnp.bfloat16
    n_dev = n_fs * n_tp
    toks, width = tokens.shape
    _, gr, gc = gate_proj.shape
    _, dr, dc = down_proj.shape
    inner = gc * n_tp
    chunks, wide = dc // lanes, n_tp * lanes
    vmem = pl.BlockSpec(memory_space=pltpu.VMEM)
    hbm = pl.BlockSpec(memory_space=pltpu.HBM)
    dma = pltpu.SemaphoreType.DMA
    new_gate, new_up, new_down, perm, returned = pl.pallas_call(
        functools.partial(fused_kernel, n_fs, n_tp),
        out_shape=(
            pltpu.VMEM((width, inner), bf16),
            pltpu.VMEM((width, inner), bf16),
            pltpu.VMEM((inner, width), bf16),
            pltpu.VMEM((toks, toks), bf16),
            pltpu.VMEM((chunks, toks, wide), bf16),
        ),
        in_specs=[hbm] * 7,
        out_specs=(vmem,) * 5,
        scratch_shapes=[
            pltpu.VMEM(tokens.shape, bf16),
            pltpu.VMEM((2, toks), jnp.int32),
            pltpu.VMEM((2, toks), f32),
            pltpu.VMEM((1, gr), f32),
            pltpu.VMEM((n_dev, gr, gc), f32),
            pltpu.VMEM((n_dev, gr, gc), f32),
            pltpu.VMEM((n_dev, dr, dc), f32),
            pltpu.VMEM((n_dev, gr, gc), bf16),
            pltpu.VMEM((n_dev, gr, gc), bf16),
            pltpu.VMEM((n_dev, dr, dc), bf16),
            pltpu.VMEM((2, 2, gr, gc), f32),
            pltpu.VMEM((2, 2, gr, gc), bf16),
            pltpu.VMEM((toks, width), bf16),
            pltpu.VMEM((n_tp, toks, width), bf16),
            pltpu.VMEM((n_fs, 1, lanes), f32),
            pltpu.VMEM((n_tp, n_fs, 1, lanes), f32),
            pltpu.VMEM((n_tp, toks, lanes), f32),
            pltpu.VMEM((n_tp, toks, inner), bf16),
            pltpu.VMEM((chunks, 2, toks, wide), f32),
            pltpu.VMEM((chunks, 2, toks, wide), bf16),
            pltpu.VMEM((chunks, 2, toks, wide), bf16),
            pltpu.VMEM((chunks, toks, wide), bf16),
            pltpu.VMEM((chunks, toks, wide), bf16),
            pltpu.VMEM((chunks, toks, wide), bf16),
            dma((4,)), dma((3, n_fs)), dma((1 + chunks + last_cuts,)), dma((1 + chunks + last_cuts,)), dma, dma, dma, dma,
            dma((3,)), dma((3,)), dma((chunks,)), dma((chunks,)), dma((chunks, 4)),
            dma((chunks, 4)), dma, dma, dma((2, 2)), pltpu.SemaphoreType.REGULAR,
        ],
        compiler_params=pltpu.CompilerParams(
            collective_id=0, has_side_effects=True, vmem_limit_bytes=47 * 1024 * 1024
        ),
    )(*(
        pltpu.with_memory_space_constraint(a, pltpu.HBM)
        for a in (
            tokens, expert_ids.T, route_weight.T, norm_gain[None, :], gate_proj, up_proj, down_proj
        )
    ))
    mixed, new_gate, new_up, new_down = pl.pallas_call(
        write_kernel,
        out_shape=(
            jax.ShapeDtypeStruct((toks, width), bf16),
            jax.ShapeDtypeStruct((width, inner), bf16),
            jax.ShapeDtypeStruct((width, inner), bf16),
            jax.ShapeDtypeStruct((inner, width), bf16),
        ),
        in_specs=[vmem] * 5,
        out_specs=(hbm,) * 4,
        scratch_shapes=[pltpu.VMEM((toks, width), bf16), dma((4,))],
        compiler_params=pltpu.CompilerParams(vmem_limit_bytes=16 * 1024 * 1024),
    )(perm, returned, new_gate, new_up, new_down)
    return mixed, new_gate[None], new_up[None], new_down[None]


def shards(n_fs, n_tp, *args):
    tokens, _, gate_proj, _, down_proj = args[:5]
    toks, experts = tokens.shape[0], gate_proj.shape[0]
    whole_tiles = (
        n_tp == group_size
        and experts == n_fs * n_tp
        and toks % (16 * n_fs) == 0
        and n_fs % 4 == 0
        and gate_proj.shape[2] % 128 == 0
        and down_proj.shape[2] % 128 == 0
        and gate_proj.shape[1] % 16 == 0
        and down_proj.shape[1] % (16 * last_cuts) == 0
        and 2 * group_size * toks == lanes * n_fs
    )
    if whole_tiles:
        return shards_fused(n_fs, n_tp, *args)
    return shards_plain(*args)


def solution(mesh):
    in_specs = (
        P(("fs", "tp"), None),
        P("fs"),
        P(None, "fs", "tp"),
        P(None, "fs", "tp"),
        P(None, "fs", "tp"),
        P(("fs", "tp"), None),
        P(("fs", "tp"), None),
    )
    out_specs = (
        P(("fs", "tp"), None),
        P(("fs", "tp"), None, None),
        P(("fs", "tp"), None, None),
        P(("fs", "tp"), None, None),
    )
    body = functools.partial(shards, mesh.shape["fs"], mesh.shape["tp"])
    return jax.shard_map(body, mesh=mesh, in_specs=in_specs, out_specs=out_specs, check_vma=False)
```

```python
import functools

import jax
import jax.numpy as jnp
from jax import lax
from jax.experimental import pallas as pl
from jax.experimental.pallas import tpu as pltpu
from jax.sharding import PartitionSpec as P

norm_eps = 1e-06
group_size = 4
lanes = 128
last_cuts = 2
MESH = pl.DeviceIdType.MESH


def shards_plain(tokens, norm_gain, gate_proj, up_proj, down_proj, expert_ids, route_weight):
    row_scale = norm_gain[None, :, None]
    gate_low = (gate_proj * row_scale).astype(jnp.bfloat16)
    up_low = (up_proj * row_scale).astype(jnp.bfloat16)
    down_low = down_proj.astype(jnp.bfloat16)
    width_fs = lax.axis_size("fs")
    width_tp = lax.axis_size("tp")

    def expand(matrix):
        return matrix.reshape((matrix.shape[0], 1) + matrix.shape[1:])

    def assemble(pieces):
        row_count, col_count = (pieces.shape[2], pieces.shape[3])
        tiled = pieces.reshape(width_fs, width_tp, row_count, col_count).transpose(0, 2, 1, 3)
        return tiled.reshape(1, width_fs * row_count, width_tp * col_count)

    arrived = (
        lax.all_to_all(expand(gate_low), ("fs", "tp"), split_axis=0, concat_axis=1, tiled=True),
        lax.all_to_all(expand(up_low), ("fs", "tp"), split_axis=0, concat_axis=1, tiled=True),
        lax.all_to_all(expand(down_low), ("fs", "tp"), split_axis=0, concat_axis=1, tiled=True),
    )
    new_gate, new_up, new_down = (assemble(arrived[0]), assemble(arrived[1]), assemble(arrived[2]))
    tok_count, width = tokens.shape
    experts = gate_proj.shape[0]
    slot_cap = 4 * tok_count // experts
    widened = tokens.astype(jnp.float32)
    normed = (
        widened * lax.rsqrt(jnp.mean(widened * widened, axis=-1, keepdims=True) + norm_eps)
    ).astype(jnp.bfloat16)
    flat_ids = expert_ids.reshape(-1)
    onehot = (flat_ids[:, None] == jnp.arange(experts, dtype=jnp.int32)[None, :]).astype(jnp.int32)
    slot_rank = jnp.sum(jnp.cumsum(onehot, axis=0) * onehot, axis=1) - 1
    slot_index = flat_ids * slot_cap + slot_rank
    source = (
        jnp.zeros((experts * slot_cap,), jnp.int32)
        .at[slot_index]
        .set(jnp.arange(2 * tok_count, dtype=jnp.int32) // 2 + 1)
    )
    filled = source > 0
    outgoing = jnp.where(
        filled[:, None], normed[jnp.maximum(source - 1, 0)], jnp.zeros((), jnp.bfloat16)
    )
    outgoing = outgoing.reshape(experts, slot_cap, width)
    arrived_rows = lax.all_to_all(outgoing, ("fs", "tp"), split_axis=0, concat_axis=0, tiled=True)
    flat_rows = arrived_rows.reshape(-1, width)
    gate_act = jnp.dot(flat_rows, new_gate[0], preferred_element_type=jnp.float32)
    up_act = jnp.dot(flat_rows, new_up[0], preferred_element_type=jnp.float32)
    hidden = (jax.nn.silu(gate_act) * up_act).astype(jnp.bfloat16)
    results = jnp.dot(hidden, new_down[0], preferred_element_type=jnp.float32).astype(jnp.bfloat16)
    returned = lax.all_to_all(
        results.reshape(arrived_rows.shape), ("fs", "tp"), split_axis=0, concat_axis=0, tiled=True
    )
    picked = returned.reshape(experts * slot_cap, width)[slot_index].reshape(tok_count, 2, width)
    mixed = jnp.sum(route_weight[:, :, None] * picked.astype(jnp.float32), axis=1).astype(
        jnp.bfloat16
    )
    return (mixed, new_gate, new_up, new_down)


def fused_kernel(
    n_fs, n_tp,
    x_in, ids_in, rw_in, gain_in, gate_in, up_in, down_in,
    gate_w, up_w, down_w, perm, fin_rx,
    x_ref, ids_ref, rw_ref, gain_ref,
    gate_st, up_st, down_st, gate_tx, up_tx, down_tx, early_st, early_tx,
    tok_tx, rows, wt_tx, wt_rx, wcol, hidden, own,
    part_tx, part_rx, sum_tx, sum_rx, fin_tx,
    in_sem, ld_sem, early_sem, met_sem, sent, w_recv, tok_recv, wt_recv, ex_recv, red_recv,
    y_recv, fin_recv,
):
    f32, bf16 = jnp.float32, jnp.bfloat16
    fs, tp = lax.axis_index("fs"), lax.axis_index("tp")
    core = lax.rem(tp, 2)
    pair = tp // 2
    partner = tp + 1 - 2 * core
    across = lax.rem(tp + 2, n_tp)
    n_dev = n_fs * n_tp
    toks, width = x_ref.shape
    per = toks // n_fs
    d_rows, d_cols = down_in.shape[1:]
    chunks = d_cols // lanes
    srcs = (gate_in, up_in, down_in)
    stages = (gate_st, up_st, down_st)
    txs = (gate_tx, up_tx, down_tx)
    lands = (gate_w, up_w, down_w)

    quarter = n_fs // 4
    layer, col = fs // quarter, lax.rem(fs, quarter)
    plane = quarter * n_tp
    barrier = pltpu.get_barrier_semaphore()

    def greet_plane(sem):
        @pl.loop(1, plane)
        def _(k):
            at = lax.rem(col * n_tp + tp + k, plane)
            pl.semaphore_signal(
                sem, inc=1,
                device_id=(layer * quarter + at // n_tp, lax.rem(at, n_tp)),
                device_id_type=MESH,
            )

    for k in range(1, 4):
        pl.semaphore_signal(
            barrier, inc=1,
            device_id=(lax.rem(layer + k, 4) * quarter + col, tp), device_id_type=MESH,
        )
    greet_plane(barrier)
    half = layer // 2
    inner_far, outer_far, mate = 2 - half, 3 - 3 * half, 4 * half + 1 - layer

    def targets(layers):
        return [
            (at * quarter + lax.rem(col + 1 + i, quarter), at is layer and i == quarter - 1,
             i == quarter - 1 and at is not layer and at is not mate)
            for i in range(quarter)
            for at in layers
        ]

    far, close = targets((outer_far, inner_far)), targets((mate, layer))
    ahead = 1
    batches = (far[:ahead], close, far[ahead:])
    plan = far[:ahead] + close + far[ahead:]
    first_of = {0: 0, ahead: 1, ahead + len(close): 2}

    def load(m, tgt, batch):
        at = pl.ds(tgt * n_tp, n_tp)
        return pltpu.make_async_copy(srcs[m].at[at], stages[m].at[at], ld_sem.at[m, batch])

    small = [
        pltpu.make_async_copy(src, dst, in_sem.at[i])
        for i, (src, dst) in enumerate(
            ((gain_in, gain_ref), (x_in, x_ref), (ids_in, ids_ref), (rw_in, rw_ref))
        )
    ]
    early = [(m, j) for j in range(2) for m in (0, 1)]
    lines = (inner_far * quarter + col, outer_far * quarter + col)

    def load_early(m, j):
        return pltpu.make_async_copy(
            srcs[m].at[lines[j] * n_tp + tp], early_st.at[m, j], early_sem
        )

    small[0].start()
    for m, j in early:
        load_early(m, j).start()
    for m in (0, 1):
        load(m, plan[0][0], 0).start()

    lane_id = lax.broadcasted_iota(jnp.int32, (toks, lanes), 1)
    row_id = lax.broadcasted_iota(jnp.int32, (toks, lanes), 0)
    in_group = lax.rem(row_id, per)
    span_lanes = group_size * per

    def as_columns(flat):
        spread_rows = jnp.concatenate([flat] * (8 // flat.shape[0]), axis=0)
        return jnp.transpose(spread_rows)

    def span(i):
        return pl.ds(pl.multiple_of(i * per, per), per)

    def all_sent(part, sem):
        pltpu.make_async_copy(part, part, sem).wait()

    def all_here(land, sem):
        pltpu.make_async_copy(land, land, sem).wait()

    small[0].wait()
    gain = jnp.broadcast_to(as_columns(gain_ref[...])[:, 0:1], gate_in.shape[1:])

    def cast(ms, tgt):
        for m in ms:

            @pl.loop(0, n_tp)
            def _(t):
                block = stages[m][tgt * n_tp + t]
                if m < 2:
                    block = block * gain
                txs[m][tgt * n_tp + t] = block.astype(bf16)

    def block_at(m):
        r, c = srcs[m].shape[1:]
        return lands[m].at[pl.ds(pl.multiple_of(fs * r, r), r), pl.ds(pl.multiple_of(tp * c, c), c)]

    def send(tgt, same, begun):
        for t in range(1 if same or begun else 0, n_tp):
            to = lax.rem(tp + t, n_tp)
            for m in (0, 1):
                pltpu.make_async_remote_copy(
                    src_ref=txs[m].at[tgt * n_tp + to], dst_ref=block_at(m),
                    send_sem=sent, recv_sem=w_recv.at[m],
                    device_id=(tgt, to), device_id_type=MESH,
                ).start()
        if same:
            for m in (0, 1):
                pltpu.make_async_copy(
                    txs[m].at[fs * n_tp + tp], block_at(m), w_recv.at[m]
                ).start()

    def loaded(m, batch, count):
        all_here(stages[m].at[pl.ds(0, count * n_tp)], ld_sem.at[m, batch])

    def step_plan(first, last):
        for k in range(first, last):
            if k in first_of:
                for m in (0, 1):
                    loaded(m, first_of[k], len(batches[first_of[k]]))
            if k < len(plan):
                cast((0, 1), plan[k][0])
            if k > 0:
                send(*plan[k - 1])

    cuts = [(k, 0, d_rows) for k in range(chunks - 1)]
    cuts += [(chunks - 1, i * d_rows // last_cuts, d_rows // last_cuts) for i in range(last_cuts)]

    def send_cut(c):
        k, row, count = cuts[c]
        piece_of = (pl.ds(row, count), pl.ds(k * lanes, lanes))
        land = down_w.at[
            pl.ds(pl.multiple_of(fs * d_rows + row, count), count),
            pl.ds(pl.multiple_of(tp * d_cols + k * lanes, lanes), lanes),
        ]
        for tgt, same, _ in close + far:
            for t in range(1 if same else 0, n_tp):
                to = lax.rem(tp + t, n_tp)
                pltpu.make_async_remote_copy(
                    src_ref=down_tx.at[(tgt * n_tp + to,) + piece_of], dst_ref=land,
                    send_sem=sent, recv_sem=w_recv.at[2 + c],
                    device_id=(tgt, to), device_id_type=MESH,
                ).start()
            if same:
                pltpu.make_async_copy(
                    down_tx.at[(fs * n_tp + tp,) + piece_of], land, w_recv.at[2 + c]
                ).start()

    all_here(early_st, early_sem)
    for m, j in early:
        early_tx[m, j] = (early_st[m, j] * gain).astype(bf16)
    pl.semaphore_wait(barrier, plane + 2)
    greet_plane(met_sem)
    for m, j in early:
        pltpu.make_async_remote_copy(
            src_ref=early_tx.at[m, j], dst_ref=block_at(m),
            send_sem=sent, recv_sem=w_recv.at[m],
            device_id=(lines[j], tp), device_id_type=MESH,
        ).start()
    step_plan(0, 1)
    for copy in small[1:]:
        copy.start()
    for m, batch in ((0, 1), (0, 2), (2, 0)):
        for tgt, _, _ in batches[batch] if m == 0 else plan:
            for n in (0, 1) if m == 0 else (2,):
                load(n, tgt, batch).start()
    pl.semaphore_wait(met_sem, plane - 1)
    step_plan(1, ahead + 1)

    for copy in small[1:]:
        copy.wait()
    x = x_ref[...].astype(f32)
    scale = lax.rsqrt(jnp.mean(x * x, axis=-1, keepdims=True) + norm_eps)
    normed = (x * scale).astype(bf16)
    idf = as_columns(ids_ref[...].astype(f32))
    grp = jnp.floor((idf + 0.5) * (1.0 / group_size))
    slot = lax.broadcasted_iota(jnp.int32, (toks, toks), 1).astype(f32)
    tok = lax.broadcasted_iota(jnp.int32, (toks, toks), 0).astype(f32)
    slot_grp = jnp.floor((slot + 0.5) * (1.0 / per))
    named = (grp[:, 0:1] == slot_grp).astype(f32)
    before = (slot < tok).astype(f32)
    rank = jnp.dot(before.astype(bf16), named.astype(bf16), preferred_element_type=f32)
    place = jnp.where(rank == slot - slot_grp * per, named, 0.0).astype(bf16)
    perm[...] = place
    by_slot = (((0,), (0,)), ((), ()))
    tok_tx[...] = lax.dot_general(
        place, normed, by_slot, preferred_element_type=f32
    ).astype(bf16)

    @pl.loop(1, n_fs)
    def _(j):
        tgt = lax.rem(fs + j, n_fs)
        pltpu.make_async_remote_copy(
            src_ref=tok_tx.at[span(tgt)], dst_ref=rows.at[tp, span(fs)],
            send_sem=sent, recv_sem=tok_recv,
            device_id=(tgt, tp), device_id_type=MESH,
        ).start()

    pltpu.make_async_copy(tok_tx.at[span(fs)], rows.at[tp, span(fs)], tok_recv).start()

    lane_pick = (lax.rem(lane_id, span_lanes) // per).astype(f32)
    local = idf - grp * group_size
    rw = as_columns(rw_ref[...])
    wv = jnp.where(local[:, 0:1] == lane_pick, rw[:, 0:1], 0.0) + jnp.where(
        local[:, 1:2] == lane_pick, rw[:, 1:2], 0.0
    )
    high = wv.astype(bf16).astype(f32)
    aug = jnp.where(lane_id < span_lanes, high, wv - high).astype(bf16)
    by_row = lax.dot_general(place, aug, by_slot, preferred_element_type=f32)
    by_row = jnp.where(lax.rem(lane_id, per) == in_group, by_row, 0.0)
    wt_tx[...] = jnp.sum(by_row.reshape(n_fs, per, lanes), axis=1, keepdims=True)

    @pl.loop(1, n_dev)
    def _(k):
        dev = lax.rem(fs * n_tp + tp + k, n_dev)
        tgt = dev // n_tp
        pltpu.make_async_remote_copy(
            src_ref=wt_tx.at[tgt], dst_ref=wt_rx.at[tp, fs],
            send_sem=sent, recv_sem=wt_recv,
            device_id=(tgt, lax.rem(dev, n_tp)), device_id_type=MESH,
        ).start()

    pltpu.make_async_copy(wt_tx.at[fs], wt_rx.at[tp, fs], wt_recv).start()

    step_plan(ahead + 1, len(plan) + 1)
    loaded(2, 0, len(plan))
    for tgt, _, _ in plan:
        cast((2,), tgt)
    for c in range(len(cuts)):
        send_cut(c)

    def swap(src, dst, to, recv_sem):
        return pltpu.make_async_remote_copy(
            src_ref=src, dst_ref=dst, send_sem=sent, recv_sem=recv_sem,
            device_id=(fs, to), device_id_type=MESH,
        )

    all_here(rows.at[tp], tok_recv)
    cross = swap(rows.at[tp], rows.at[tp], across, ex_recv.at[0])
    cross.start()
    near = swap(rows.at[tp], rows.at[tp], partner, ex_recv.at[1])
    near.start()
    cross.wait_recv()
    other = swap(rows.at[across], rows.at[across], partner, ex_recv.at[2])
    other.start()
    near.wait_recv()
    other.wait_recv()
    all_here(wt_rx, wt_recv)
    mine = lax.rem(lane_id, span_lanes) == tp * per + in_group

    @pl.loop(0, n_tp)
    def _(q):
        w = jnp.broadcast_to(wt_rx[q], (n_fs, per, lanes)).reshape(toks, lanes)
        wcol[q] = jnp.broadcast_to(
            jnp.sum(jnp.where(mine, w, 0.0), axis=-1, keepdims=True), (toks, lanes)
        )

    for m in (0, 1):
        all_here(lands[m], w_recv.at[m])

    @pl.loop(0, n_tp)
    def _(q):
        g = jnp.dot(rows[q], gate_w[...], preferred_element_type=f32)
        u = jnp.dot(rows[q], up_w[...], preferred_element_type=f32)
        hidden[q] = (g / (1.0 + jnp.exp(-g)) * u).astype(bf16)

    pieces = 4
    step = n_fs // pieces

    def piece(p):
        return lax.rem(half * 2 + 2 + p, pieces)

    def piece_rows(p):
        return pl.ds(pl.multiple_of(piece(p) * step * per, step * per), step * per)

    def reduce_near(k):
        return swap(part_tx.at[k], part_rx.at[k], partner, red_recv.at[k])

    def over(k, p):
        at = piece_rows(p)
        return swap(
            sum_tx.at[k, at], sum_rx.at[k, at], across, y_recv.at[k, p if k == chunks - 1 else min(p, 1)]
        )

    def multiply(k):
        columns = jnp.concatenate(
            [down_w[:, pl.ds(t * d_cols + k * lanes, lanes)] for t in range(n_tp)], axis=1
        )

        def partial(q):
            w = jnp.concatenate([wcol[q]] * n_tp, axis=1)
            return jnp.dot(hidden[q], columns, preferred_element_type=f32) * w

        for side in range(2):
            part_tx[k, side] = partial(side * 2 + 1 - core).astype(bf16)
        reduce_near(k).start()
        own[k, 0] = partial((1 - pair) * 2 + core)
        own[k, 1] = partial(pair * 2 + core)

    def cross_over(k):
        reduce_near(k).wait_recv()
        for p in range(pieces):
            at = piece_rows(p)
            sum_tx[k, at] = (own[k, 0, at] + part_rx[k, 1 - pair, at].astype(f32)).astype(bf16)
            over(k, p).start()

    def give_back(k, ps=tuple(range(4))):
        for p in ps:
            at = piece_rows(p)
            own_part = own[k, 1, at] + part_rx[k, pair, at].astype(f32)
            if k == chunks - 1 or p == 0:
                over(k, p).wait_recv()
            elif p == 1:
                rest = sum_rx.at[k, pl.ds(0, toks - step * per)]
                all_here(rest, y_recv.at[k, 1])
            fin_tx[k, at] = (own_part + sum_rx[k, at].astype(f32)).astype(bf16)
            for i in range(step):
                to = piece(p) * step + i

                @pl.when(to != fs)
                def _():
                    pltpu.make_async_remote_copy(
                        src_ref=fin_tx.at[k, span(to)], dst_ref=fin_rx.at[k, span(fs)],
                        send_sem=sent, recv_sem=fin_recv,
                        device_id=(to, tp), device_id_type=MESH,
                    ).start()

                @pl.when(to == fs)
                def _():
                    pltpu.make_async_copy(
                        fin_tx.at[k, span(fs)], fin_rx.at[k, span(fs)], fin_recv
                    ).start()

    def cut_here(c):
        area = down_w.at[pl.ds(0, n_fs * cuts[c][2]), pl.ds(0, n_tp * lanes)]
        all_here(area, w_recv.at[2 + c])

    for k in range(chunks - 1):
        cut_here(k)
        multiply(k)
        cross_over(k)
    last = chunks - 1
    cut_here(last)
    give_back(0)
    give_back(1, (0,))
    cut_here(last + 1)
    multiply(last)
    cross_over(last)
    give_back(last - 1, (0,))
    give_back(last, (0,))
    for k in range(1, chunks):
        give_back(k, (1, 2, 3))

    for tx in txs:
        all_sent(tx.at[pl.ds(0, n_dev - 1)], sent)
    all_sent(tok_tx.at[pl.ds(0, toks - per)], sent)
    all_sent(wt_rx.at[0, pl.ds(0, n_fs - 1)], sent)
    for _ in range(n_tp - 1):
        all_sent(wt_rx.at[0], sent)
    all_sent(rows.at[pl.ds(0, 3)], sent)
    all_sent(part_tx, sent)
    all_sent(sum_tx, sent)
    all_sent(fin_tx.at[:, pl.ds(0, toks - per)], sent)
    all_here(fin_rx, fin_recv)


def write_kernel(perm, fin_rx, gate, up, down, mixed_out, gate_out, up_out, down_out, mixed, sem):
    chunks, _, wide = fin_rx.shape
    blocks = wide // lanes
    moves = ((gate, gate_out), (up, up_out), (down, down_out), (mixed, mixed_out))

    def put(m):
        return pltpu.make_async_copy(moves[m][0], moves[m][1], sem.at[m])

    for m in range(3):
        put(m).start()
    for k in range(chunks):
        part = jnp.dot(
            perm[...], fin_rx[k], preferred_element_type=jnp.float32
        ).astype(jnp.bfloat16)
        for t in range(blocks):
            mixed[:, pl.ds((t * chunks + k) * lanes, lanes)] = part[:, t * lanes:(t + 1) * lanes]
    put(3).start()
    for m in range(4):
        put(m).wait()


def shards_fused(n_fs, n_tp, tokens, norm_gain, gate_proj, up_proj, down_proj, expert_ids, route_weight):
    f32, bf16 = jnp.float32, jnp.bfloat16
    n_dev = n_fs * n_tp
    toks, width = tokens.shape
    _, gr, gc = gate_proj.shape
    _, dr, dc = down_proj.shape
    inner = gc * n_tp
    chunks, wide = dc // lanes, n_tp * lanes
    vmem = pl.BlockSpec(memory_space=pltpu.VMEM)
    hbm = pl.BlockSpec(memory_space=pltpu.HBM)
    dma = pltpu.SemaphoreType.DMA
    new_gate, new_up, new_down, perm, returned = pl.pallas_call(
        functools.partial(fused_kernel, n_fs, n_tp),
        out_shape=(
            pltpu.VMEM((width, inner), bf16),
            pltpu.VMEM((width, inner), bf16),
            pltpu.VMEM((inner, width), bf16),
            pltpu.VMEM((toks, toks), bf16),
            pltpu.VMEM((chunks, toks, wide), bf16),
        ),
        in_specs=[hbm] * 7,
        out_specs=(vmem,) * 5,
        scratch_shapes=[
            pltpu.VMEM(tokens.shape, bf16),
            pltpu.VMEM((2, toks), jnp.int32),
            pltpu.VMEM((2, toks), f32),
            pltpu.VMEM((1, gr), f32),
            pltpu.VMEM((n_dev, gr, gc), f32),
            pltpu.VMEM((n_dev, gr, gc), f32),
            pltpu.VMEM((n_dev, dr, dc), f32),
            pltpu.VMEM((n_dev, gr, gc), bf16),
            pltpu.VMEM((n_dev, gr, gc), bf16),
            pltpu.VMEM((n_dev, dr, dc), bf16),
            pltpu.VMEM((2, 2, gr, gc), f32),
            pltpu.VMEM((2, 2, gr, gc), bf16),
            pltpu.VMEM((toks, width), bf16),
            pltpu.VMEM((n_tp, toks, width), bf16),
            pltpu.VMEM((n_fs, 1, lanes), f32),
            pltpu.VMEM((n_tp, n_fs, 1, lanes), f32),
            pltpu.VMEM((n_tp, toks, lanes), f32),
            pltpu.VMEM((n_tp, toks, inner), bf16),
            pltpu.VMEM((chunks, 2, toks, wide), f32),
            pltpu.VMEM((chunks, 2, toks, wide), bf16),
            pltpu.VMEM((chunks, 2, toks, wide), bf16),
            pltpu.VMEM((chunks, toks, wide), bf16),
            pltpu.VMEM((chunks, toks, wide), bf16),
            pltpu.VMEM((chunks, toks, wide), bf16),
            dma((4,)), dma((3, 3)), dma, pltpu.SemaphoreType.REGULAR, dma,
            dma((1 + chunks + last_cuts,)), dma, dma, dma((3,)), dma((chunks,)),
            dma((chunks, 4)), dma,
        ],
        compiler_params=pltpu.CompilerParams(
            collective_id=0, has_side_effects=True, vmem_limit_bytes=47 * 1024 * 1024
        ),
    )(*(
        pltpu.with_memory_space_constraint(a, pltpu.HBM)
        for a in (
            tokens, expert_ids.T, route_weight.T, norm_gain[None, :], gate_proj, up_proj, down_proj
        )
    ))
    mixed, new_gate, new_up, new_down = pl.pallas_call(
        write_kernel,
        out_shape=(
            jax.ShapeDtypeStruct((toks, width), bf16),
            jax.ShapeDtypeStruct((width, inner), bf16),
            jax.ShapeDtypeStruct((width, inner), bf16),
            jax.ShapeDtypeStruct((inner, width), bf16),
        ),
        in_specs=[vmem] * 5,
        out_specs=(hbm,) * 4,
        scratch_shapes=[pltpu.VMEM((toks, width), bf16), dma((4,))],
        compiler_params=pltpu.CompilerParams(vmem_limit_bytes=16 * 1024 * 1024),
    )(perm, returned, new_gate, new_up, new_down)
    return mixed, new_gate[None], new_up[None], new_down[None]


def shards(n_fs, n_tp, *args):
    tokens, _, gate_proj, _, down_proj = args[:5]
    toks, experts = tokens.shape[0], gate_proj.shape[0]
    whole_tiles = (
        n_tp == group_size
        and experts == n_fs * n_tp
        and toks % (16 * n_fs) == 0
        and n_fs % 4 == 0
        and gate_proj.shape[2] % 128 == 0
        and down_proj.shape[2] % 128 == 0
        and gate_proj.shape[1] % 16 == 0
        and down_proj.shape[1] % (16 * last_cuts) == 0
        and 2 * group_size * toks == lanes * n_fs
    )
    if whole_tiles:
        return shards_fused(n_fs, n_tp, *args)
    return shards_plain(*args)


def solution(mesh):
    in_specs = (
        P(("fs", "tp"), None),
        P("fs"),
        P(None, "fs", "tp"),
        P(None, "fs", "tp"),
        P(None, "fs", "tp"),
        P(("fs", "tp"), None),
        P(("fs", "tp"), None),
    )
    out_specs = (
        P(("fs", "tp"), None),
        P(("fs", "tp"), None, None),
        P(("fs", "tp"), None, None),
        P(("fs", "tp"), None, None),
    )
    body = functools.partial(shards, mesh.shape["fs"], mesh.shape["tp"])
    return jax.shard_map(body, mesh=mesh, in_specs=in_specs, out_specs=out_specs, check_vma=False)
```
